256 devices in a mesh: rep: 2 (over z_hi), fs: 16 (over z_lo, y), tp: 8 (over x, core).
Axes of the slice: x: 4, y: 4, z: 8 (z_hi: 2, z_lo: 4; z = z_hi * 4 + z_lo), core: 2. Of those that a mesh axis runs over, the one named last changes fastest.
Arguments:
- stream: bfloat16 [32, 1024, 2048], P(('rep', 'fs'), None, 'tp'), may hold values from -6 to 6
- norm_gain: float32 [2048], replicated, may hold values from 0.1 to 1.9
- w_in: float32 [2048, 512], P('fs', 'tp'), may hold values from -0.125 to 0.125
- s_in: float32 [512], P(('tp', 'fs')), may hold values from 0.1 to 1.9
- pool_w: bfloat16 [4, 128, 128], replicated, may hold values from -0.5 to 0.5
- w_out: float32 [512, 2048], P('fs', 'tp'), may hold values from -0.25 to 0.25
- s_out: float32 [2048], P(('tp', 'fs')), may hold values from 0.1 to 1.9
- ffn_gain: float32 [2048], replicated, may hold values from 0.1 to 1.9
- w_up: float32 [2048, 8192], P('fs', 'tp'), may hold values from -0.125 to 0.125
- s_up: float32 [8192], P(('tp', 'fs')), may hold values from 0.1 to 1.9
- w_down: float32 [8192, 2048], P('tp', 'fs'), may hold values from -0.0625 to 0.0625
- s_down: float32 [2048], P('fs'), may hold values from 0.1 to 1.9
Outputs:
- result: bfloat16 [32, 1024, 2048], P(('rep', 'fs'), None, 'tp')
The draws below stay inside these ranges and needn't reach their ends.
All inputs are finite; a program needn't handle non-finite values.
Results may differ from the reference program's by a relative error of at most 0.012.
Values may be sent and summed in bfloat16 or wider, within the bound.
No kernel may reach another device: no remote copies, remote signals or barrier semaphores. Data moves between devices by JAX's collectives and lax.ppermute only.
A program may use at most 64 MiB of HBM per device.

```python
import jax
import jax.numpy as jnp
from jax import lax

D = 2048
FF = 8192
PW = 512
GROUP = 128
SEQ_LEN = 1024
BATCH = 32
N_TP = 8


def block_scale(stream_key, shape, cuts, least, top_value):
    level, own = 1.0, jax.random.fold_in(stream_key, 6)
    for axis_at, shards_of in cuts:
        draws = jnp.exp(jax.random.uniform(jax.random.fold_in(own, axis_at), (shards_of,), jnp.float32, least / len(cuts), top_value / len(cuts)))
        level = level * jnp.repeat(draws, shape[axis_at] // shards_of).reshape([-1 if axis == axis_at else 1 for axis in range(len(shape))])
    return level


def bell_draw(key, shape, scale, limit, shards=(), kind=jnp.bfloat16):
    entries = jax.random.normal(key, shape, jnp.float32) * scale
    if len(shards) > 0:
        entries = block_scale(key, shape, shards, -0.22, 0.18) * entries
    return jnp.clip(entries, min=-limit, max=limit).astype(kind)


def setup_inputs(seed: int = 0) -> dict:
    key_list = jax.random.split(jax.random.key(seed), 13)
    return {
        "stream": bell_draw(key_list[0], (BATCH, SEQ_LEN, D), 1.0, 6.0, ((0, 32), (2, 8))),
        "norm_gain": jnp.clip(1.0 + 0.18 * jax.random.normal(key_list[1], (D,), jnp.float32), 0.1, 1.9),
        "w_in": bell_draw(key_list[2], (D, PW), D ** -0.5, 0.125, ((0, 16), (1, 8)), jnp.float32),
        "s_in": jnp.clip(1.0 + 0.18 * jax.random.normal(key_list[3], (PW,), jnp.float32), 0.1, 1.9),
        "pool_w": bell_draw(key_list[4], (4, GROUP, GROUP), GROUP ** -0.5, 0.5),
        "w_out": bell_draw(key_list[5], (PW, D), PW ** -0.5, 0.25, ((0, 16), (1, 8)), jnp.float32),
        "s_out": jnp.clip(1.0 + 0.18 * jax.random.normal(key_list[6], (D,), jnp.float32), 0.1, 1.9),
        "ffn_gain": jnp.clip(1.0 + 0.18 * jax.random.normal(key_list[7], (D,), jnp.float32), 0.1, 1.9),
        "w_up": bell_draw(key_list[8], (D, FF), D ** -0.5, 0.125, ((0, 16), (1, 8)), jnp.float32),
        "s_up": jnp.clip(1.0 + 0.18 * jax.random.normal(key_list[9], (FF,), jnp.float32), 0.1, 1.9),
        "w_down": bell_draw(key_list[10], (FF, D), FF ** -0.5, 0.0625, ((0, 8), (1, 16)), jnp.float32),
        "s_down": jnp.clip(1.0 + 0.18 * jax.random.normal(key_list[11], (D,), jnp.float32), 0.1, 1.9),
    }


epsilon = 0.25

def rms_rows(values, gain):
    floats = values.astype(jnp.float32)
    scale = lax.rsqrt(lax.optimization_barrier(jnp.mean(floats * floats, axis=-1, keepdims=True)) + epsilon)
    return (floats * scale * gain).astype(jnp.bfloat16)

def pool_sequence(pool_in):
    length = pool_in.shape[0]
    floats = pool_in.astype(jnp.float32)
    running = jnp.concatenate([jnp.zeros((1, floats.shape[1]), jnp.float32), jnp.cumsum(floats, axis=0)], axis=0)
    positions = jnp.arange(length, dtype=jnp.int32)
    pieces = []
    for level in range(4):
        half = 2 ** level
        lower = jnp.clip(positions - half, 0, length).astype(jnp.int32)
        upper = jnp.clip(positions + half, 0, length).astype(jnp.int32)
        part = running[:, level * GROUP:(level + 1) * GROUP]
        counts = (upper - lower).astype(jnp.float32)[:, None]
        pieces.append((part[upper] - part[lower]) / counts - floats[:, level * GROUP:(level + 1) * GROUP])
    return jnp.concatenate(pieces, axis=1).astype(jnp.bfloat16)

def one_sequence(tokens, norm_gain, w_in, s_in, pool_w, w_out, s_out, ffn_gain, w_up, s_up, w_down, s_down):
    length = tokens.shape[0]
    normed = rms_rows(tokens, norm_gain)
    pool_in = (jnp.dot(normed, w_in.astype(jnp.bfloat16), preferred_element_type=jnp.float32) * s_in).astype(jnp.bfloat16)
    pooled = pool_sequence(pool_in)
    grouped = jnp.einsum('lgc,gcd->lgd', pooled.reshape(length, 4, GROUP).astype(jnp.float32), pool_w.astype(jnp.float32))
    grouped = grouped.reshape(length, PW).astype(jnp.bfloat16)
    branch = jnp.dot(grouped, w_out.astype(jnp.bfloat16), preferred_element_type=jnp.float32) * s_out
    mixed = (tokens.astype(jnp.float32) + branch).astype(jnp.bfloat16)
    ffn_in = rms_rows(mixed, ffn_gain)
    upward = jnp.dot(ffn_in, w_up.astype(jnp.bfloat16), preferred_element_type=jnp.float32) * s_up
    hidden = jnp.square(jax.nn.relu(upward)).astype(jnp.bfloat16)
    block = FF // N_TP
    hidden_blocks = hidden.reshape(length, N_TP, block).astype(jnp.float32)
    down_blocks = w_down.astype(jnp.bfloat16).reshape(N_TP, block, D).astype(jnp.float32)
    partials = jnp.einsum('ljf,jfd->jld', hidden_blocks, down_blocks) * s_down
    rounded = lax.optimization_barrier(partials.astype(jnp.bfloat16))
    summed = lax.optimization_barrier(jnp.sum(rounded.astype(jnp.float32), axis=0))
    return (mixed.astype(jnp.float32) + summed).astype(jnp.bfloat16)

def reference(stream, norm_gain, w_in, s_in, pool_w, w_out, s_out, ffn_gain, w_up, s_up, w_down, s_down):

    def single(tokens):
        return one_sequence(tokens, norm_gain, w_in, s_in, pool_w, w_out, s_out, ffn_gain, w_up, s_up, w_down, s_down)
    return lax.map(single, stream)
```

```python
import functools

import jax
import jax.numpy as jnp
from jax import lax
from jax.experimental import pallas as pl
from jax.experimental.pallas import tpu as pltpu
from jax.sharding import Mesh
from jax.sharding import PartitionSpec as P


BF = jnp.bfloat16
F32 = jnp.float32
EPS = 0.25
SEQ = 1024
FS = ("z", "y")
TP = ("x", "c")
VMEM = pl.BlockSpec(memory_space=pltpu.VMEM)


def send(array, axes, shift):
    count = lax.axis_size(axes)
    return lax.ppermute(array, axes, [(i, (i + shift) % count) for i in range(count)])


def swapped(array):
    return send(array, "c", 1)


def put(whole, part, at):
    return lax.dynamic_update_index_in_dim(whole, part, at, 0)


def two_parts(values):
    high = values.astype(BF)
    return high, (values - high.astype(F32)).astype(BF)


def widened(row, lanes):
    return jnp.pad(row, (0, lanes - row.shape[0]))[None]


def dot(a, b):
    return jnp.dot(a, b, preferred_element_type=F32)


def dot_t(a, b):
    return lax.dot_general(a, b, (((1,), (1,)), ((), ())), preferred_element_type=F32)


def around(at):
    return [at] + [lax.rem(at + step, 4) for step in (3, 1, 2)]


def owners():
    x, c = lax.axis_index("x"), lax.axis_index("c")
    return [2 * chip + c for chip in around(x)] + [2 * chip + 1 - c for chip in around(x)]


def call(kernel, out_shape, scratch, limit_mb, flops, *args):
    moved = sum(a.size * a.dtype.itemsize for a in args)
    return pl.pallas_call(
        kernel,
        out_shape=out_shape,
        in_specs=[VMEM] * len(args),
        out_specs=jax.tree.map(lambda _: VMEM, out_shape),
        scratch_shapes=scratch,
        compiler_params=pltpu.CompilerParams(vmem_limit_bytes=limit_mb << 20),
        cost_estimate=pl.CostEstimate(flops=flops, bytes_accessed=moved, transcendentals=0),
    )(*args)


def pool_kernel(*refs):
    pieces, (mix, s_in, pool_w, out, padded) = refs[:8], refs[8:]
    x, whose = lax.axis_index("x"), owners()
    total = jnp.zeros((SEQ, 128), F32)
    squares = jnp.zeros((SEQ, 128), F32)
    for k, piece in enumerate(pieces):
        t = whose[k]
        first, second = mix[2 * t], mix[2 * t + 1]
        weight = jnp.concatenate(
            [first[32:96, :128], first[32:96, 128:], second[32:96, :128], second[32:96, 128:]], axis=0
        )
        values = piece[...]
        total += dot(values, weight)
        wide = values.astype(F32)
        wide = wide * wide
        squares += wide[:, :128] + wide[:, 128:]
    scale = lax.rsqrt(jnp.sum(squares, axis=1, keepdims=True) / 2048 + EPS)
    pool_in = (total * scale * s_in[...]).astype(BF)
    padded[0:128] = jnp.zeros((128, 128), BF)
    padded[128 : 128 + SEQ] = pool_in
    padded[128 + SEQ :] = jnp.zeros((128, 128), BF)
    half = jnp.left_shift(1, x)
    row = lax.broadcasted_iota(jnp.int32, (256, 512), 0)
    source = lax.broadcasted_iota(jnp.int32, (256, 512), 1) - 128
    band = jnp.where((source >= row - half) & (source < row + half), 1.0, 0.0).astype(BF)
    own = pool_w[x]
    for block in range(SEQ // 256):
        sums = dot(band, padded[block * 256 : block * 256 + 512])
        at = lax.broadcasted_iota(jnp.int32, (256, 128), 0) + block * 256
        counts = jnp.minimum(at + half, SEQ) - jnp.maximum(at - half, 0)
        here = padded[128 + block * 256 : 384 + block * 256].astype(F32)
        pooled = (sums / counts.astype(F32) - here).astype(BF)
        out[block * 256 : block * 256 + 256] = dot(pooled, own).astype(BF)


def mix_kernel(*refs):
    pieces, groups, weights = refs[:8], refs[8:12], refs[12:20]
    mixed, own, factor = refs[20:]
    chips, whose = around(lax.axis_index("x")), owners()
    for block in range(2):
        rows = pl.ds(block * 512, 512)
        squares = jnp.zeros((512, 128), F32)
        left = jnp.concatenate([g[rows, :] for g in groups], axis=1)
        for k in range(8):
            t = whose[k]
            weight = jnp.concatenate(
                [weights[k][pl.ds(pl.multiple_of(chips[j] * 128, 128), 128), :] for j in range(4)],
                axis=0,
            )
            scale = weights[k][512:513, :].astype(F32) + weights[k][513:514, :].astype(F32)
            value = (pieces[k][rows, :].astype(F32) + dot(left, weight) * scale).astype(BF)
            mixed[rows, pl.ds(pl.multiple_of(t * 256, 256), 256)] = value
            if k == 0:
                own[rows, :] = value
            wide = value.astype(F32)
            wide = wide * wide
            squares += wide[:, :128] + wide[:, 128:]
        mean = jnp.sum(squares, axis=1, keepdims=True) / 2048
        factor[rows, :] = jnp.broadcast_to(lax.rsqrt(mean + EPS), (512, 128))


def up_kernel(mixed, factor, s_up, b0, b1, b2, b3, b4, hidden):
    places = around(lax.axis_index("z"))
    for n in range(4):
        cols = slice(n * 256, n * 256 + 256)
        for block in range(2):
            rows = pl.ds(block * 512, 512)
            total = jnp.zeros((512, 256), F32)
            for k, bundle in enumerate((b0, b1, b2)):
                left = mixed[rows, pl.ds(pl.multiple_of(places[k] * 512, 512), 512)]
                total += dot(left, bundle[:, :, cols].reshape(512, 256))
            start = places[3] * 512
            for k, bundle in enumerate((b3, b4)):
                left = mixed[rows, pl.ds(pl.multiple_of(start + 256 * k, 256), 256)]
                total += dot(left, bundle[:, :, cols].reshape(256, 256))
            scale = jnp.concatenate([factor[rows, :]] * 2, axis=1) * s_up[:, cols]
            value = jnp.maximum(total * scale, 0.0)
            hidden[rows, cols] = (value * value).astype(BF)


def down_kernel(hidden, b0, b1, b2, b3, b4, out):
    x, c = lax.axis_index("x"), lax.axis_index("c")
    for bundle, column in zip((b0, b1, b2, None), around(lax.axis_index("y"))):
        core, side = jnp.bitwise_xor(lax.shift_right_logical(column, 1), c), jnp.bitwise_and(column, 1)
        lanes = pl.ds(pl.multiple_of(side * 128, 128), 128)
        for pair in range(2):
            weights = []
            for j in (2 * pair, 2 * pair + 1):
                chip = lax.rem(x + j, 4)
                if bundle is not None:
                    weights.append(bundle[chip])
                else:
                    inner = jnp.bitwise_and(chip, 1)
                    weights.append(jnp.where(chip < 2, b3[inner], b4[inner]))
            weight = jnp.concatenate(weights, axis=0)
            for block in range(2):
                rows = pl.ds(block * 512, 512)
                value = dot_t(hidden[rows, :], weight).astype(BF)
                out[core, 2 * pair, rows, lanes] = value[:, :128]
                out[core, 2 * pair + 1, rows, lanes] = value[:, 128:]


def on_device(
    stream, norm_gain, w_in, s_in, pool_w, w_out, s_out, ffn_gain, w_up, s_up, w_down, s_down
):
    z, y, x, c = (lax.axis_index(name) for name in ("z", "y", "x", "c"))
    f = 4 * z + y
    ring_z = ("rep", "z")
    tokens = stream[0]

    near = [send(tokens, "x", 2), send(tokens, "x", 1), send(tokens, "x", -1)]
    pieces = [tokens, near[1], near[2], near[0]]
    pieces = pieces + [swapped(p) for p in pieces]

    gain = lax.dynamic_slice(norm_gain, (f * 128,), (128,))
    w_in_own = (w_in * gain[:, None]).astype(BF)
    scale_rows = jnp.pad(jnp.stack(two_parts(s_in)), ((0, 14), (0, 60)))
    with_scale = jnp.concatenate([w_in_own, scale_rows], axis=0)
    other = swapped(with_scale)
    pair = jnp.concatenate(
        [jnp.where(c == 0, with_scale, other), jnp.where(c == 0, other, with_scale)], axis=1
    )
    out_high, out_low = two_parts(s_out)
    up_high, up_low = two_parts(s_up)
    packet = jnp.concatenate(
        [
            w_out.astype(BF),
            jnp.concatenate([pair[:64], pair[64:128]], axis=1),
            widened(out_high, 256),
            widened(out_low, 256),
            jnp.pad(pair[128:130], ((0, 0), (0, 128))),
            widened(up_high, 256),
            widened(up_low, 256),
            jnp.zeros((10, 256), BF),
        ],
        axis=0,
    )
    by_y = jnp.zeros((4, 112, 256), BF)
    from_y = [send(packet, "y", s) for s in (2, 1, -1)]
    by_y = put(by_y, packet, y)
    for part, step in zip(from_y, (2, 3, 1)):
        by_y = put(by_y, part, (y + step) % 4)
    mix = jnp.zeros((4, 4, 112, 256), BF)
    far = jnp.concatenate([send(by_y[:2], ring_z, 2), send(by_y[2:], ring_z, -2)], axis=0)
    from_z = [far, send(by_y, ring_z, 1), send(by_y, ring_z, -1)]
    mix = put(mix, by_y, z)
    for part, step in zip(from_z, (2, 3, 1)):
        mix = put(mix, part, (z + step) % 4)
    mix = mix.reshape(16, 112, 256)

    gain = lax.dynamic_slice(ffn_gain, (f * 128,), (128,))
    up_own = (w_up * gain[:, None]).astype(BF)
    up_y = jnp.zeros((4, 128, 1024), BF)
    from_y = [send(up_own, "y", s) for s in (2, 1, -1)]
    up_y = put(up_y, up_own, y)
    for part, step in zip(from_y, (2, 3, 1)):
        up_y = put(up_y, part, (y + step) % 4)
    down_own = (w_down * s_down[None]).astype(BF).T
    down_z = jnp.zeros((4, 128, 1024), BF)
    far = jnp.concatenate([send(down_own[:64], ring_z, 2), send(down_own[64:], ring_z, -2)], axis=0)
    from_z = [far, send(down_own, ring_z, 1), send(down_own, ring_z, -1)]
    down_z = put(down_z, down_own, z)
    for part, step in zip(from_z, (2, 3, 1)):
        down_z = put(down_z, part, (z + step) % 4)
    up_low_side, up_high_side = send(up_y, ring_z, 1), send(up_y, ring_z, -1)
    down_low_side, down_high_side = send(down_z, "y", 1), send(down_z, "y", -1)
    up_far = [send(up_low_side[:2], ring_z, 1), send(up_high_side[2:], ring_z, -1)]
    down_far = [send(down_low_side[:2], "y", 1), send(down_high_side[2:], "y", -1)]

    s_in_all = (mix[:, 98].astype(F32) + mix[:, 99].astype(F32)).reshape(16, 256)
    s_in_row = jnp.concatenate(
        [s_in_all[:, :4].reshape(1, 64), s_in_all[:, 64:68].reshape(1, 64)], axis=1
    )
    grouped = call(
        pool_kernel,
        jax.ShapeDtypeStruct((SEQ, 128), BF),
        [pltpu.VMEM((SEQ + 256, 128), BF)],
        24,
        800_000_000,
        *pieces,
        mix,
        s_in_row,
        pool_w,
    )
    near = [send(grouped, "x", 2), send(grouped, "x", 1), send(grouped, "x", -1)]
    groups = [grouped, near[1], near[2], near[0]]

    scales = jnp.pad(
        jnp.stack([mix[:, 96, :16].reshape(256), mix[:, 97, :16].reshape(256)]), ((0, 14), (0, 0))
    )
    out_own = jnp.concatenate([mix[:, :32].reshape(512, 256), scales], axis=0)
    near = [send(out_own, "x", 2), send(out_own, "x", 1), send(out_own, "x", -1)]
    outs = [out_own, near[1], near[2], near[0]]
    outs = outs + [swapped(w) for w in outs]
    mixed, mixed_own, factor = call(
        mix_kernel,
        (
            jax.ShapeDtypeStruct((SEQ, 2048), BF),
            jax.ShapeDtypeStruct((SEQ, 256), BF),
            jax.ShapeDtypeStruct((SEQ, 128), F32),
        ),
        [],
        40,
        2_200_000_000,
        *pieces,
        *groups,
        *outs,
    )

    s_up_row = (mix[:, 100, :64].astype(F32) + mix[:, 101, :64].astype(F32)).reshape(1, 1024)
    hidden = call(
        up_kernel,
        jax.ShapeDtypeStruct((SEQ, 1024), BF),
        [],
        40,
        4_300_000_000,
        mixed,
        factor,
        s_up_row,
        up_y,
        up_low_side,
        up_high_side,
        *up_far,
    )
    partial = call(
        down_kernel,
        jax.ShapeDtypeStruct((2, 4, SEQ, 256), BF),
        [],
        40,
        4_300_000_000,
        hidden,
        down_z,
        down_low_side,
        down_high_side,
        *down_far,
    )
    crossed = swapped(partial[1])
    chip = partial[0].astype(F32) + crossed.astype(F32)
    summed = chip[0]
    for step, shift in ((2, 2), (1, 1), (3, -1)):
        summed = summed + send(chip[step].astype(BF), "x", shift).astype(F32)
    return (mixed_own.astype(F32) + summed).astype(BF)[None]


def solution(mesh):
    finer = Mesh(
        mesh.devices.reshape(mesh.shape["rep"], 4, 4, 4, 2),
        ("rep", "z", "y", "x", "c"),
    )
    rows = ("rep", "z", "y")
    both = ("x", "c", "z", "y")
    return jax.shard_map(
        on_device,
        mesh=finer,
        in_specs=(
            P(rows, None, TP),
            P(),
            P(FS, TP),
            P(both),
            P(),
            P(FS, TP),
            P(both),
            P(),
            P(FS, TP),
            P(both),
            P(TP, FS),
            P(FS),
        ),
        out_specs=P(rows, None, TP),
        check_vma=False,
    )
```

```python
import functools

import jax
import jax.numpy as jnp
from jax import lax
from jax.experimental import pallas as pl
from jax.experimental.pallas import tpu as pltpu
from jax.sharding import Mesh
from jax.sharding import PartitionSpec as P


BF = jnp.bfloat16
F32 = jnp.float32
EPS = 0.25
SEQ = 1024
FS = ("z", "y")
TP = ("x", "c")
VMEM = pl.BlockSpec(memory_space=pltpu.VMEM)


def send(array, axes, shift):
    count = lax.axis_size(axes)
    return lax.ppermute(array, axes, [(i, (i + shift) % count) for i in range(count)])


def swapped(array):
    return send(array, "c", 1)


def two_parts(values):
    high = values.astype(BF).astype(F32)
    return high, values - high


def dot(a, b):
    return jnp.dot(a, b, preferred_element_type=F32)


def dot_t(a, b):
    return lax.dot_general(a, b, (((1,), (1,)), ((), ())), preferred_element_type=F32)


def around(at):
    return [at] + [lax.rem(at + step, 4) for step in (3, 1, 2)]


def owners():
    x, c = lax.axis_index("x"), lax.axis_index("c")
    return [2 * chip + c for chip in around(x)] + [2 * chip + 1 - c for chip in around(x)]


def call(kernel, out_shape, scratch, limit_mb, flops, *args):
    moved = sum(a.size * a.dtype.itemsize for a in args)
    return pl.pallas_call(
        kernel,
        out_shape=out_shape,
        in_specs=[VMEM] * len(args),
        out_specs=jax.tree.map(lambda _: VMEM, out_shape),
        scratch_shapes=scratch,
        compiler_params=pltpu.CompilerParams(vmem_limit_bytes=limit_mb << 20),
        cost_estimate=pl.CostEstimate(flops=flops, bytes_accessed=moved, transcendentals=0),
    )(*args)


def column_of(row):
    return jnp.broadcast_to(row, (128, 128)).T


def prep_kernel(
    norm_gain, w_in, w_in_other, s_in, s_in_other, w_out, s_out, ffn_gain, w_up, s_up, w_down, s_down,
    up, packet, top, bottom, small,
):
    c = lax.axis_index("c")
    f = 4 * lax.axis_index("z") + lax.axis_index("y")
    gain = column_of(ffn_gain[pl.ds(f, 1), :])
    for j in range(8):
        lanes = slice(j * 128, j * 128 + 128)
        up[:, lanes] = (w_up[:, lanes] * gain).astype(BF)
        packet[:128, lanes] = (w_down[lanes, :] * s_down[...]).T.astype(BF)
    gain = column_of(norm_gain[pl.ds(f, 1), :])
    mine, other = w_in[...], w_in_other[...]
    pair = jnp.concatenate(
        [jnp.where(c == 0, mine, other), jnp.where(c == 0, other, mine)], axis=1
    )
    pair = pair * gain
    for j in range(8):
        small[0:16, j * 128 : j * 128 + 128] = pair[j * 16 : j * 16 + 16]
    for j in range(4):
        small[16:24, j * 256 : j * 256 + 256] = w_out[j * 8 : j * 8 + 8, :]
    small[24:32] = jnp.zeros((8, 1024), F32)
    mine, other = s_in[...], s_in_other[...]
    rows = (
        (s_out[...], 0),
        (jnp.where(c == 0, mine, other), 256),
        (jnp.where(c == 0, other, mine), 512),
        (s_up[...], 768),
    )
    for row, at in rows:
        high, low = two_parts(row)
        small[24:25, at : at + row.shape[1]] = high
        small[24:25, at + 128 : at + 128 + row.shape[1]] = low
    packet[128:] = small[...].astype(BF)
    top[...] = packet[:80]
    bottom[...] = packet[80:]


def unpack_kernel(m0, m1, m2, m3, w_in, w_out, s_in, s_up):
    ys, zs = around(lax.axis_index("y")), around(lax.axis_index("z"))
    w_out[512:] = jnp.zeros((16, 256), BF)
    lane = lax.broadcasted_iota(jnp.int32, (16, 128), 1)
    at = lax.broadcasted_iota(jnp.int32, (16, 128), 0)
    firsts = [jnp.zeros((16, 128), F32) for _ in range(8)]
    for m, yy in zip((m0, m1, m2, m3), ys):
        for k, zz in enumerate(zs):
            f = 4 * zz + yy
            block = m[k]
            for j in range(8):
                w_in[pl.ds(pl.multiple_of(f * 128 + j * 16, 16), 16), :] = block[:16, j * 128 : j * 128 + 128]
            low = block[16:32].astype(F32)
            rows = jnp.concatenate([low[:8, j * 256 : j * 256 + 256] for j in range(4)], axis=0)
            w_out[pl.ds(pl.multiple_of(f * 32, 32), 32), :] = rows.astype(BF)
            for j in range(8):
                row = jnp.broadcast_to(low[8:9, j * 128 : j * 128 + 128], (16, 128))
                firsts[j] = jnp.where(at == f, row, firsts[j])

    def flat(rows, width):
        pieces = []
        for group in range(16 * width // 128):
            total = jnp.zeros((1, 128), F32)
            for i in range(128 // width):
                source = group * (128 // width) + i
                row = jnp.where(lane[:1] < width, rows[source : source + 1], 0.0)
                total += pltpu.roll(row, i * width, 1) if i else row
            pieces.append(total)
        return jnp.concatenate(pieces, axis=1) if len(pieces) > 1 else pieces[0]

    w_out[512:528] = jnp.concatenate(
        [flat(firsts[0], 16), flat(firsts[1], 16), jnp.zeros((14, 256), F32)], axis=0
    ).astype(BF)
    both = [firsts[2] + firsts[3], firsts[4] + firsts[5]]
    both = jnp.where(lane < 4, both[0], 0.0) + pltpu.roll(jnp.where(lane < 4, both[1], 0.0), 64, 1)
    total = jnp.zeros((1, 128), F32)
    for i in range(16):
        row = both[i : i + 1]
        total += pltpu.roll(row, 4 * i, 1) if i else row
    s_in[...] = total
    s_up[...] = flat(firsts[6] + firsts[7], 64)


def pool_kernel(*refs):
    pieces, (w_in, s_in, pool_w, out, mine, padded) = refs[:8], refs[8:]
    x, whose = lax.axis_index("x"), owners()
    first = pl.ds(pl.multiple_of(lax.axis_index("c") * 512, 512), 512)
    padded[0:128] = jnp.zeros((128, 128), BF)
    padded[128 + SEQ :] = jnp.zeros((128, 128), BF)

    @pl.loop(0, 4)
    def _(block):
        rows = pl.ds(pl.multiple_of(block * 256, 256), 256)
        total = jnp.zeros((256, 128), F32)
        squares = jnp.zeros((256, 128), F32)
        for k, piece in enumerate(pieces):
            values = piece[rows, :]
            total += dot(values, w_in[pl.ds(pl.multiple_of(whose[k] * 256, 256), 256), :])
            wide = values.astype(F32)
            wide = wide * wide
            squares += wide[:, :128] + wide[:, 128:]
        scale = lax.rsqrt(jnp.sum(squares, axis=1, keepdims=True) / 2048 + EPS)
        padded[pl.ds(pl.multiple_of(128 + block * 256, 128), 256), :] = (total * scale * s_in[...]).astype(BF)

    half = jnp.left_shift(1, x)
    row = lax.broadcasted_iota(jnp.int32, (256, 512), 0)
    source = lax.broadcasted_iota(jnp.int32, (256, 512), 1) - 128
    band = jnp.where((source >= row - half) & (source < row + half), 1.0, 0.0).astype(BF)
    own = pool_w[x]

    @pl.loop(0, 4)
    def _(block):
        sums = dot(band, padded[pl.ds(pl.multiple_of(block * 256, 256), 512), :])
        at = lax.broadcasted_iota(jnp.int32, (256, 128), 0) + block * 256
        counts = jnp.minimum(at + half, SEQ) - jnp.maximum(at - half, 0)
        here = padded[pl.ds(pl.multiple_of(128 + block * 256, 128), 256), :].astype(F32)
        pooled = (sums / counts.astype(F32) - here).astype(BF)
        out[pl.ds(pl.multiple_of(block * 256, 256), 256), :] = dot(pooled, own).astype(BF)

    mine[...] = out[first, :]


def mix_kernel(*refs):
    pieces, grouped, near, across, weights = refs[:8], refs[8], refs[9:12], refs[12:15], refs[15:23]
    mixed, own, factor = refs[23:]
    chips, whose = around(lax.axis_index("x")), owners()
    c = lax.axis_index("c")

    @pl.loop(0, 2)
    def _(block):
        rows = pl.ds(pl.multiple_of(block * 512, 512), 512)
        squares = jnp.zeros((512, 128), F32)
        left = jnp.concatenate(
            [grouped[rows, :]] + [jnp.where(block == c, a[...], b[...]) for a, b in zip(near, across)],
            axis=1,
        )
        for k in range(8):
            weight = jnp.concatenate(
                [weights[k][pl.ds(pl.multiple_of(chips[j] * 128, 128), 128), :] for j in range(4)],
                axis=0,
            )
            scale = weights[k][512:513, :].astype(F32) + weights[k][513:514, :].astype(F32)
            value = (pieces[k][rows, :].astype(F32) + dot(left, weight) * scale).astype(BF)
            mixed[rows, pl.ds(pl.multiple_of(whose[k] * 256, 256), 256)] = value
            if k == 0:
                own[rows, :] = value
            wide = value.astype(F32)
            wide = wide * wide
            squares += wide[:, :128] + wide[:, 128:]
        mean = jnp.sum(squares, axis=1, keepdims=True) / 2048
        factor[rows, :] = jnp.broadcast_to(lax.rsqrt(mean + EPS), (512, 128))


def up_kernel(mixed, factor, s_up, *refs):
    parts, hidden = refs[:8], refs[8]
    ys, zs = around(lax.axis_index("y")), around(lax.axis_index("z"))

    @pl.loop(0, 8)
    def _(step):
        rows = pl.ds(pl.multiple_of(lax.rem(step, 2) * 512, 512), 512)
        cols = pl.ds(pl.multiple_of(lax.div(step, 2) * 256, 256), 256)
        total = jnp.zeros((512, 256), F32)
        for k in range(8):
            left = [
                mixed[rows, pl.ds(pl.multiple_of((4 * zs[k // 2] + ys[2 * (k % 2) + i]) * 128, 128), 128)]
                for i in range(2)
            ]
            total += dot(jnp.concatenate(left, axis=1), parts[k][:, :, cols].reshape(256, 256))
        scale = jnp.concatenate([factor[rows, :]] * 2, axis=1) * s_up[:, cols]
        value = jnp.maximum(total * scale, 0.0)
        hidden[rows, cols] = (value * value).astype(BF)


def down_kernel(column, hidden, a0, a1, b0, b1, own, other):
    x, c = lax.axis_index("x"), lax.axis_index("c")
    zs = around(lax.axis_index("z"))
    place = around(lax.axis_index("y"))[column]
    is_own = lax.shift_right_logical(place, 1) == c
    for k, (a, b) in enumerate(((a0, b0), (a1, b1))):
        chips = [lax.rem(zs[2 * k + i] - x + 4, 4) for i in range(2)]
        first, second = a[...].reshape(256, 1024), b[...].reshape(256, 1024)
        for out, weight in ((other, jnp.where(is_own, second, first)), (own, jnp.where(is_own, first, second))):

            @pl.loop(0, 2)
            def _(block, out=out, weight=weight):
                rows = pl.ds(pl.multiple_of(block * 512, 512), 512)
                value = dot_t(hidden[rows, :], weight).astype(BF)
                out[chips[0], rows, :] = value[:, :128]
                out[chips[1], rows, :] = value[:, 128:]


def in_halves(top, bottom, axes):
    low_top, high_bottom = send(top, axes, 1), send(bottom, axes, -1)
    low_bottom, high_top = send(bottom, axes, 1), send(top, axes, -1)
    return low_top, low_bottom, high_top, high_bottom, send(low_top, axes, 1), send(high_bottom, axes, -1)


def near_three(array):
    far = send(array, "x", 2)
    return [send(array, "x", 1), send(array, "x", -1), far]


def on_device(
    stream, norm_gain, w_in, s_in, pool_w, w_out, s_out, ffn_gain, w_up, s_up, w_down, s_down
):
    y = lax.axis_index("y")
    ring_z = ("rep", "z")
    tokens = stream[0]
    s_in = s_in[None]

    pieces = [tokens] + near_three(tokens)
    pieces = pieces + [swapped(p) for p in pieces]

    def bf(*shape):
        return jax.ShapeDtypeStruct(shape, BF)

    def f32(*shape):
        return jax.ShapeDtypeStruct(shape, F32)

    up, packet, top, bottom = call(
        prep_kernel,
        (bf(128, 1024), bf(160, 1024), bf(80, 1024), bf(80, 1024)),
        [pltpu.VMEM((32, 1024), F32)],
        12,
        1_000_000,
        norm_gain.reshape(16, 128),
        w_in,
        swapped(w_in),
        s_in,
        swapped(s_in),
        w_out,
        s_out[None],
        ffn_gain.reshape(16, 128),
        w_up,
        s_up[None],
        w_down,
        s_down[None],
    )
    low, high = send(packet, ring_z, 1), send(packet, ring_z, -1)
    far_top, far_bottom = send(top, ring_z, 2), send(bottom, ring_z, -2)
    up_far, up_low, up_high = send(up, "y", 2), send(up, "y", 1), send(up, "y", -1)

    mixer = jnp.stack([packet[128:], low[128:], high[128:], far_bottom[48:]])
    far = send(mixer, "y", 2)
    w_in_all, out_own, s_in_row, s_up_row = call(
        unpack_kernel,
        (bf(2048, 128), bf(528, 256), f32(1, 128), f32(1, 1024)),
        [],
        8,
        1_000_000,
        mixer,
        send(mixer, "y", 1),
        send(mixer, "y", -1),
        far,
    )
    up_parts = [jnp.stack([up, up_low]), jnp.stack([up_high, up_far])]
    up_parts += in_halves(*up_parts, ring_z)
    down_parts = [
        jnp.stack([packet[:128], low[:128]]),
        jnp.stack([high[:128], jnp.concatenate([far_top, far_bottom[:48]], axis=0)]),
    ]
    down_parts += in_halves(*down_parts, "y")

    grouped, mine = call(
        pool_kernel,
        (bf(SEQ, 128), bf(512, 128)),
        [pltpu.VMEM((SEQ + 256, 128), BF)],
        16,
        800_000_000,
        *pieces,
        w_in_all,
        s_in_row,
        pool_w,
    )
    near = near_three(mine)
    outs = [out_own] + near_three(out_own)
    outs = outs + [swapped(w) for w in outs]
    mixed, mixed_own, factor = call(
        mix_kernel,
        (bf(SEQ, 2048), bf(SEQ, 256), f32(SEQ, 128)),
        [],
        32,
        2_200_000_000,
        *pieces,
        grouped,
        *near,
        *[swapped(g) for g in near],
        *outs,
    )

    hidden = call(
        up_kernel,
        bf(SEQ, 1024),
        [],
        32,
        4_300_000_000,
        mixed,
        factor,
        s_up_row,
        *up_parts,
    )
    sums = []
    for first, second in ((1, 2), (0, 3)):
        own, other = call(
            functools.partial(down_kernel, first),
            (bf(4, SEQ, 128), bf(4, SEQ, 128)),
            [],
            32,
            2_200_000_000,
            hidden,
            *down_parts[2 * first : 2 * first + 2],
            *down_parts[2 * second : 2 * second + 2],
        )
        chip = own.astype(F32) + swapped(other).astype(F32)
        total = chip[0]
        for step, shift in ((2, 2), (1, 1), (3, -1)):
            total = total + send(chip[step].astype(BF), "x", shift).astype(F32)
        sums.append(total)
    beside, here = sums
    odd = jnp.bitwise_and(y, 1) == 1
    summed = jnp.concatenate(
        [jnp.where(odd, beside, here), jnp.where(odd, here, beside)], axis=1
    )
    return (mixed_own.astype(F32) + summed).astype(BF)[None]


def solution(mesh):
    finer = Mesh(
        mesh.devices.reshape(mesh.shape["rep"], 4, 4, 4, 2),
        ("rep", "z", "y", "x", "c"),
    )
    rows = ("rep", "z", "y")
    both = ("x", "c", "z", "y")
    return jax.shard_map(
        on_device,
        mesh=finer,
        in_specs=(
            P(rows, None, TP),
            P(),
            P(FS, TP),
            P(both),
            P(),
            P(FS, TP),
            P(both),
            P(),
            P(FS, TP),
            P(both),
            P(TP, FS),
            P(FS),
        ),
        out_specs=P(rows, None, TP),
        check_vma=False,
    )
```

```python
import functools

import jax
import jax.numpy as jnp
from jax import lax
from jax.experimental import pallas as pl
from jax.experimental.pallas import tpu as pltpu
from jax.sharding import Mesh
from jax.sharding import PartitionSpec as P


BF = jnp.bfloat16
F32 = jnp.float32
EPS = 0.25
SEQ = 1024
FS = ("z", "y")
TP = ("x", "c")
VMEM = pl.BlockSpec(memory_space=pltpu.VMEM)


def send(array, axes, shift):
    count = lax.axis_size(axes)
    return lax.ppermute(array, axes, [(i, (i + shift) % count) for i in range(count)])


def swapped(array):
    return send(array, "c", 1)


def two_parts(values):
    high = values.astype(BF).astype(F32)
    return high, values - high


def dot(a, b):
    return jnp.dot(a, b, preferred_element_type=F32)


def dot_t(a, b):
    return lax.dot_general(a, b, (((1,), (1,)), ((), ())), preferred_element_type=F32)


def around(at):
    return [at] + [lax.rem(at + step, 4) for step in (3, 1, 2)]


def owners():
    x, c = lax.axis_index("x"), lax.axis_index("c")
    return [2 * chip + c for chip in around(x)] + [2 * chip + 1 - c for chip in around(x)]


def call(kernel, out_shape, scratch, limit_mb, flops, *args, in_hbm=0):
    moved = sum(a.size * a.dtype.itemsize for a in args)
    return pl.pallas_call(
        kernel,
        out_shape=out_shape,
        in_specs=[VMEM] * (len(args) - in_hbm) + [pl.BlockSpec(memory_space=pltpu.HBM)] * in_hbm,
        out_specs=jax.tree.map(lambda _: VMEM, out_shape),
        scratch_shapes=scratch,
        compiler_params=pltpu.CompilerParams(vmem_limit_bytes=limit_mb << 20),
        cost_estimate=pl.CostEstimate(flops=flops, bytes_accessed=moved, transcendentals=0),
    )(*args)


def column_of(row):
    return jnp.broadcast_to(row, (128, 128)).T


def prep_kernel(
    w_in, w_in_other, norm_gain_at, w_out_at, s_out_at, ffn_gain_at, w_up_at, s_up_at, w_down_at, s_down_at,
    up, packet, top, bottom, small, norm_gain, w_out, s_out, ffn_gain, w_up, s_up, w_down, s_down, done,
):
    sources = (w_up_at, ffn_gain_at, w_down_at, s_down_at, norm_gain_at, w_out_at, s_out_at, s_up_at)
    targets = (w_up, ffn_gain, w_down, s_down, norm_gain, w_out, s_out, s_up)
    copies = [pltpu.make_async_copy(a, b, done.at[k]) for k, (a, b) in enumerate(zip(sources, targets))]
    for copy in copies:
        copy.start()
    for copy in copies:
        copy.wait()
    c = lax.axis_index("c")
    f = 4 * lax.axis_index("z") + lax.axis_index("y")
    gain = column_of(ffn_gain[pl.ds(f, 1), :])
    for j in range(8):
        lanes = slice(j * 128, j * 128 + 128)
        up[:, lanes] = (w_up[:, lanes] * gain).astype(BF)
        packet[:128, lanes] = (w_down[lanes, :] * s_down[...]).T.astype(BF)
    gain = column_of(norm_gain[pl.ds(f, 1), :])
    mine, other = w_in[:128], w_in_other[:128]
    pair = jnp.concatenate(
        [jnp.where(c == 0, mine, other), jnp.where(c == 0, other, mine)], axis=1
    )
    pair = pair * gain
    for j in range(8):
        small[0:16, j * 128 : j * 128 + 128] = pair[j * 16 : j * 16 + 16]
    for j in range(4):
        small[16:24, j * 256 : j * 256 + 256] = w_out[j * 8 : j * 8 + 8, :]
    small[24:32] = jnp.zeros((8, 1024), F32)
    mine, other = w_in[128:129, :4], w_in_other[128:129, :4]
    rows = (
        (s_out[...], 0),
        (jnp.where(c == 0, mine, other), 256),
        (jnp.where(c == 0, other, mine), 512),
        (s_up[...], 768),
    )
    for row, at in rows:
        high, low = two_parts(row)
        small[24:25, at : at + row.shape[1]] = high
        small[24:25, at + 128 : at + 128 + row.shape[1]] = low
    packet[128:] = small[...].astype(BF)
    top[...] = packet[:80]
    bottom[...] = packet[80:]


def unpack_kernel(m0, m1, m2, m3, w_in, w_out, s_in, s_up):
    ys, zs = around(lax.axis_index("y")), around(lax.axis_index("z"))
    w_out[512:] = jnp.zeros((16, 256), BF)
    lane = lax.broadcasted_iota(jnp.int32, (16, 128), 1)
    at = lax.broadcasted_iota(jnp.int32, (16, 128), 0)
    firsts = [jnp.zeros((16, 128), F32) for _ in range(8)]
    for m, yy in zip((m0, m1, m2, m3), ys):
        for k, zz in enumerate(zs):
            f = 4 * zz + yy
            block = m[k]
            for j in range(8):
                w_in[pl.ds(pl.multiple_of(f * 128 + j * 16, 16), 16), :] = block[:16, j * 128 : j * 128 + 128]
            low = block[16:32].astype(F32)
            rows = jnp.concatenate([low[:8, j * 256 : j * 256 + 256] for j in range(4)], axis=0)
            w_out[pl.ds(pl.multiple_of(f * 32, 32), 32), :] = rows.astype(BF)
            for j in range(8):
                row = jnp.broadcast_to(low[8:9, j * 128 : j * 128 + 128], (16, 128))
                firsts[j] = jnp.where(at == f, row, firsts[j])

    def flat(rows, width):
        pieces = []
        for group in range(16 * width // 128):
            total = jnp.zeros((1, 128), F32)
            for i in range(128 // width):
                source = group * (128 // width) + i
                row = jnp.where(lane[:1] < width, rows[source : source + 1], 0.0)
                total += pltpu.roll(row, i * width, 1) if i else row
            pieces.append(total)
        return jnp.concatenate(pieces, axis=1) if len(pieces) > 1 else pieces[0]

    w_out[512:528] = jnp.concatenate(
        [flat(firsts[0], 16), flat(firsts[1], 16), jnp.zeros((14, 256), F32)], axis=0
    ).astype(BF)
    both = [firsts[2] + firsts[3], firsts[4] + firsts[5]]
    both = jnp.where(lane < 4, both[0], 0.0) + pltpu.roll(jnp.where(lane < 4, both[1], 0.0), 64, 1)
    total = jnp.zeros((1, 128), F32)
    for i in range(16):
        row = both[i : i + 1]
        total += pltpu.roll(row, 4 * i, 1) if i else row
    s_in[...] = total
    s_up[...] = flat(firsts[6] + firsts[7], 64)


def piece_refs(refs):
    return list(refs[:5]) + [refs[5].at[k] for k in range(3)]


def pool_kernel(*refs):
    pieces, (w_in, s_in, pool_w, out, mine, padded) = piece_refs(refs), refs[6:]
    x, whose = lax.axis_index("x"), owners()
    first = pl.ds(pl.multiple_of(lax.axis_index("c") * 512, 512), 512)
    padded[0:128] = jnp.zeros((128, 128), BF)
    padded[128 + SEQ :] = jnp.zeros((128, 128), BF)

    @pl.loop(0, 4)
    def _(block):
        rows = pl.ds(pl.multiple_of(block * 256, 256), 256)
        total = jnp.zeros((256, 128), F32)
        squares = jnp.zeros((256, 128), F32)
        for k, piece in enumerate(pieces):
            values = piece[rows, :]
            total += dot(values, w_in[pl.ds(pl.multiple_of(whose[k] * 256, 256), 256), :])
            wide = values.astype(F32)
            wide = wide * wide
            squares += wide[:, :128] + wide[:, 128:]
        scale = lax.rsqrt(jnp.sum(squares, axis=1, keepdims=True) / 2048 + EPS)
        padded[pl.ds(pl.multiple_of(128 + block * 256, 128), 256), :] = (total * scale * s_in[...]).astype(BF)

    half = jnp.left_shift(1, x)
    row = lax.broadcasted_iota(jnp.int32, (256, 512), 0)
    source = lax.broadcasted_iota(jnp.int32, (256, 512), 1) - 128
    band = jnp.where((source >= row - half) & (source < row + half), 1.0, 0.0).astype(BF)
    own = pool_w[x]

    @pl.loop(0, 4)
    def _(block):
        sums = dot(band, padded[pl.ds(pl.multiple_of(block * 256, 256), 512), :])
        at = lax.broadcasted_iota(jnp.int32, (256, 128), 0) + block * 256
        counts = jnp.minimum(at + half, SEQ) - jnp.maximum(at - half, 0)
        here = padded[pl.ds(pl.multiple_of(128 + block * 256, 128), 256), :].astype(F32)
        pooled = (sums / counts.astype(F32) - here).astype(BF)
        out[pl.ds(pl.multiple_of(block * 256, 256), 256), :] = dot(pooled, own).astype(BF)

    mine[...] = out[first, :]


def mix_kernel(*refs):
    pieces, grouped, near, across = piece_refs(refs), refs[6], refs[7:10], refs[10]
    weights = list(refs[11:15]) + [refs[15].at[k] for k in range(4)]
    mixed, own, factor = refs[16:]
    chips, whose = around(lax.axis_index("x")), owners()
    c = lax.axis_index("c")

    @pl.loop(0, 2)
    def _(block):
        rows = pl.ds(pl.multiple_of(block * 512, 512), 512)
        squares = jnp.zeros((512, 128), F32)
        left = jnp.concatenate(
            [grouped[rows, :]] + [jnp.where(block == c, a[...], across[k]) for k, a in enumerate(near)],
            axis=1,
        )
        for k in range(8):
            weight = jnp.concatenate(
                [weights[k][pl.ds(pl.multiple_of(chips[j] * 128, 128), 128), :] for j in range(4)],
                axis=0,
            )
            scale = weights[k][512:513, :].astype(F32) + weights[k][513:514, :].astype(F32)
            value = (pieces[k][rows, :].astype(F32) + dot(left, weight) * scale).astype(BF)
            mixed[rows, pl.ds(pl.multiple_of(whose[k] * 256, 256), 256)] = value
            if k == 0:
                own[rows, :] = value
            wide = value.astype(F32)
            wide = wide * wide
            squares += wide[:, :128] + wide[:, 128:]
        mean = jnp.sum(squares, axis=1, keepdims=True) / 2048
        factor[rows, :] = jnp.broadcast_to(lax.rsqrt(mean + EPS), (512, 128))


def up_kernel(mixed, factor, s_up, b0, b1, b2, b3, b4, hidden):
    ys, zs = around(lax.axis_index("y")), around(lax.axis_index("z"))
    parts = [b.at[pl.ds(2 * k, 2)] for b in (b0, b1, b2) for k in range(2)] + [b3, b4]

    @pl.loop(0, 8)
    def _(step):
        rows = pl.ds(pl.multiple_of(lax.rem(step, 2) * 512, 512), 512)
        cols = pl.ds(pl.multiple_of(lax.div(step, 2) * 256, 256), 256)
        total = jnp.zeros((512, 256), F32)
        for k in range(8):
            left = [
                mixed[rows, pl.ds(pl.multiple_of((4 * zs[k // 2] + ys[2 * (k % 2) + i]) * 128, 128), 128)]
                for i in range(2)
            ]
            total += dot(jnp.concatenate(left, axis=1), parts[k][:, :, cols].reshape(256, 256))
        scale = jnp.concatenate([factor[rows, :]] * 2, axis=1) * s_up[:, cols]
        value = jnp.maximum(total * scale, 0.0)
        hidden[rows, cols] = (value * value).astype(BF)


def down_kernel(steps, hidden, b0, b1, b2, b3, b4, own, other):
    x, y, z = (lax.axis_index(name) for name in ("x", "y", "z"))
    core = lax.shift_right_logical(y, 1)
    y_is_own = core == lax.axis_index("c")
    low_is_own = y_is_own == (jnp.bitwise_and(y, 1) == 1)
    side = jnp.bitwise_and(y, 1)

    @pl.loop(0, 2 * len(steps))
    def _(step):
        rows = pl.ds(pl.multiple_of(lax.rem(step, 2) * 512, 512), 512)
        k = lax.div(step, 2)
        chip = lax.rem(x + (lax.rem(2 * k + 1, 5) if len(steps) > 1 else steps[0]), 4)
        away = lax.rem(chip - z + 4, 4)
        place = jnp.where(away == 0, 0, jnp.where(away == 1, 2, jnp.where(away == 2, 3, 1)))
        inner = jnp.bitwise_and(place, 1)
        far = jnp.where(place < 2, b3[inner], b4[inner])
        for first, second, first_is_own, lane in (
            (b0[place], far, y_is_own, side),
            (b1[place], b2[place], low_is_own, 1 - side),
        ):
            weight = jnp.concatenate(
                [jnp.where(first_is_own, second, first), jnp.where(first_is_own, first, second)], axis=0
            )
            value = dot_t(hidden[rows, :], weight).astype(BF)
            lanes = pl.ds(pl.multiple_of(lane * 128, 128), 128)
            other[k, rows, lanes] = value[:, :128]
            own[k, rows, lanes] = value[:, 128:]


def along(bundle, axes):
    low, high = send(bundle, axes, 1), send(bundle, axes, -1)
    return [bundle, low, high, send(low[:2], axes, 1), send(high[2:], axes, -1)]


def near_three(array):
    far = send(array, "x", 2)
    return [send(array, "x", 1), send(array, "x", -1), far]


def bf(*shape):
    return jax.ShapeDtypeStruct(shape, BF)


def f32(*shape):
    return jax.ShapeDtypeStruct(shape, F32)


def layer(
    stream, norm_gain, w_in, s_in, pool_w, w_out, s_out, ffn_gain, w_up, s_up, w_down, s_down
):
    ring_z = ("rep", "z")
    tokens = stream[0]

    near = near_three(tokens)
    pieces = [tokens] + near
    both_in = jnp.concatenate([w_in, jnp.pad(s_in[None], ((0, 7), (0, 60)))], axis=0)
    other_in = swapped(both_in)
    pieces.append(swapped(tokens))
    pieces.append(swapped(jnp.stack(near)))

    arrays = (
        both_in,
        other_in,
        norm_gain.reshape(16, 128),
        w_out,
        s_out[None],
        ffn_gain.reshape(16, 128),
        w_up,
        s_up[None],
        w_down,
        s_down[None],
    )
    up, packet, top, bottom = call(
        prep_kernel,
        (bf(128, 1024), bf(160, 1024), bf(80, 1024), bf(80, 1024)),
        [pltpu.VMEM((32, 1024), F32)]
        + [pltpu.VMEM(a.shape, F32) for a in arrays[2:]]
        + [pltpu.SemaphoreType.DMA((8,))],
        60,
        1_000_000,
        *arrays,
        in_hbm=8,
    )
    low, high = send(packet, ring_z, 1), send(packet, ring_z, -1)
    far_top, far_bottom = send(top, ring_z, 2), send(bottom, ring_z, -2)
    up_far, up_low, up_high = send(up, "y", 2), send(up, "y", 1), send(up, "y", -1)

    mixer = jnp.stack([packet[128:], low[128:], high[128:], far_bottom[48:]])
    far = send(mixer, "y", 2)
    mixers = [mixer, send(mixer, "y", 1), send(mixer, "y", -1), far]
    w_in_all, out_own, s_in_row, s_up_row = call(
        unpack_kernel,
        (bf(2048, 128), bf(528, 256), f32(1, 128), f32(1, 1024)),
        [],
        8,
        1_000_000,
        *mixers,
    )
    up_parts = along(jnp.stack([up, up_low, up_high, up_far]), ring_z)
    down_parts = along(
        jnp.stack(
            [
                packet[:128],
                low[:128],
                high[:128],
                jnp.concatenate([far_top, far_bottom[:48]], axis=0),
            ]
        ),
        "y",
    )

    grouped, mine = call(
        pool_kernel,
        (bf(SEQ, 128), bf(512, 128)),
        [pltpu.VMEM((SEQ + 256, 128), BF)],
        16,
        800_000_000,
        *pieces,
        w_in_all,
        s_in_row,
        pool_w,
    )
    near = near_three(mine)
    across = swapped(jnp.stack(near))
    outs = [out_own] + near_three(out_own)
    outs.append(swapped(jnp.stack(outs)))
    mixed, mixed_own, factor = call(
        mix_kernel,
        (bf(SEQ, 2048), bf(SEQ, 256), f32(SEQ, 128)),
        [],
        32,
        2_200_000_000,
        *pieces,
        grouped,
        *near,
        across,
        *outs,
    )

    hidden = call(
        up_kernel, bf(SEQ, 1024), [], 32, 4_300_000_000, mixed, factor, s_up_row, *up_parts
    )
    chips = []
    for steps in ((2,), (1, 3, 0)):
        count = len(steps)
        own, other = call(
            functools.partial(down_kernel, steps),
            (bf(count, SEQ, 256), bf(count, SEQ, 256)),
            [],
            32,
            1_075_000_000 * count,
            hidden,
            *down_parts,
        )
        crossed = swapped(other)
        chips += [own[k].astype(F32) + crossed[k].astype(F32) for k in range(count)]
    total = mixed_own.astype(F32) + chips[3]
    for k, shift in enumerate((2, 1, -1)):
        total = total + send(chips[k].astype(BF), "x", shift).astype(F32)
    return total.astype(BF)[None]


def solution(mesh):
    finer = Mesh(
        mesh.devices.reshape(mesh.shape["rep"], 4, 4, 4, 2),
        ("rep", "z", "y", "x", "c"),
    )
    rows = ("rep", "z", "y")
    both = ("x", "c", "z", "y")
    return jax.shard_map(
        layer,
        mesh=finer,
        in_specs=(
            P(rows, None, TP),
            P(),
            P(FS, TP),
            P(both),
            P(),
            P(FS, TP),
            P(both),
            P(),
            P(FS, TP),
            P(both),
            P(TP, FS),
            P(FS),
        ),
        out_specs=P(rows, None, TP),
        check_vma=False,
    )
```

```python
import functools

import jax
import jax.numpy as jnp
from jax import lax
from jax.experimental import pallas as pl
from jax.experimental.pallas import tpu as pltpu
from jax.sharding import Mesh
from jax.sharding import PartitionSpec as P


BF = jnp.bfloat16
F32 = jnp.float32
EPS = 0.25
SEQ = 1024
FS = ("z", "y")
TP = ("x", "c")
VMEM = pl.BlockSpec(memory_space=pltpu.VMEM)


def send(array, axes, shift):
    count = lax.axis_size(axes)
    return lax.ppermute(array, axes, [(i, (i + shift) % count) for i in range(count)])


def swapped(array):
    return send(array, "c", 1)


def two_parts(values):
    high = values.astype(BF).astype(F32)
    return high, values - high


def dot(a, b):
    return jnp.dot(a, b, preferred_element_type=F32)


def dot_t(a, b):
    return lax.dot_general(a, b, (((1,), (1,)), ((), ())), preferred_element_type=F32)


def around(at):
    return [at] + [lax.rem(at + step, 4) for step in (3, 1, 2)]


def owners():
    x, c = lax.axis_index("x"), lax.axis_index("c")
    return [2 * chip + c for chip in around(x)] + [2 * chip + 1 - c for chip in around(x)]


def call(kernel, out_shape, scratch, limit_mb, flops, *args, in_hbm=0):
    moved = sum(a.size * a.dtype.itemsize for a in args)
    return pl.pallas_call(
        kernel,
        out_shape=out_shape,
        in_specs=[VMEM] * (len(args) - in_hbm) + [pl.BlockSpec(memory_space=pltpu.HBM)] * in_hbm,
        out_specs=jax.tree.map(lambda _: VMEM, out_shape),
        scratch_shapes=scratch,
        compiler_params=pltpu.CompilerParams(vmem_limit_bytes=limit_mb << 20),
        cost_estimate=pl.CostEstimate(flops=flops, bytes_accessed=moved, transcendentals=0),
    )(*args)


def column_of(row):
    return jnp.broadcast_to(row, (128, 128)).T


def prep_kernel(
    norm_gain_at, w_in_at, s_in_at, w_out_at, s_out_at, ffn_gain_at, w_up_at, s_up_at, w_down_at, s_down_at,
    mixer, up, down, small, norm_gain, w_in, s_in, w_out, s_out, ffn_gain, w_up, s_up, w_down, s_down, done,
):
    sources = (norm_gain_at, w_in_at, s_in_at, w_out_at, s_out_at, s_up_at, ffn_gain_at, w_up_at, w_down_at, s_down_at)
    targets = (norm_gain, w_in, s_in, w_out, s_out, s_up, ffn_gain, w_up, w_down, s_down)
    copies = [pltpu.make_async_copy(a, b, done.at[k]) for k, (a, b) in enumerate(zip(sources, targets))]
    for copy in copies:
        copy.start()
    for copy in copies[:6]:
        copy.wait()
    f = 4 * lax.axis_index("z") + lax.axis_index("y")
    own = jnp.concatenate([w_in[...]] * 2, axis=0).T * column_of(norm_gain[pl.ds(f, 1), :])
    low_lanes = lax.broadcasted_iota(jnp.int32, (8, 128), 1) < 64
    for j in range(8):
        lanes = slice(j * 128, j * 128 + 128)
        small[0:8, lanes] = jnp.where(low_lanes, own[j * 16 : j * 16 + 8], own[j * 16 + 8 : j * 16 + 16])
    for j in range(4):
        small[8:16, j * 256 : j * 256 + 256] = w_out[j * 8 : j * 8 + 8, :]
    small[16:24] = jnp.zeros((8, 1024), F32)
    for row, at in ((s_out[...], 0), (s_in[...], 256), (s_up[...], 512)):
        high, low = two_parts(row)
        small[16:17, at : at + row.shape[1]] = high
        small[16:17, at + 128 : at + 128 + row.shape[1]] = low
    mixer[...] = small[...].astype(BF)
    for copy in copies[6:]:
        copy.wait()
    gain = column_of(ffn_gain[pl.ds(f, 1), :])
    for j in range(8):
        lanes = slice(j * 128, j * 128 + 128)
        up[:, lanes] = (w_up[:, lanes] * gain).astype(BF)
        down[:, lanes] = (w_down[lanes, :] * s_down[...]).T.astype(BF)


def unpack_kernel(m0, m1, m2, m3, w_in, w_out, s_up):
    ys, zs = around(lax.axis_index("y")), around(lax.axis_index("z"))
    lane = lax.broadcasted_iota(jnp.int32, (16, 128), 1)
    at = lax.broadcasted_iota(jnp.int32, (16, 128), 0)
    low_lanes = lane[:8] < 64
    firsts = [jnp.zeros((16, 128), F32) for _ in range(6)]
    for m, yy in zip((m0, m1, m2, m3), ys):
        for k, zz in enumerate(zs):
            f = 4 * zz + yy
            block = m[k].astype(F32)
            for j in range(8):
                part = block[:8, j * 128 : j * 128 + 128]
                turned = pltpu.roll(part, 64, 1)
                rows = jnp.concatenate(
                    [jnp.where(low_lanes, part, turned), jnp.where(low_lanes, turned, part)], axis=0
                )
                w_in[pl.ds(pl.multiple_of(f * 128 + j * 16, 16), 16), :] = rows.astype(BF)
            rows = jnp.concatenate([block[8:16, j * 256 : j * 256 + 256] for j in range(4)], axis=0)
            w_out[pl.ds(pl.multiple_of(f * 32, 32), 32), :] = rows.astype(BF)
            for j in range(6):
                row = jnp.broadcast_to(block[16:17, j * 128 : j * 128 + 128], (16, 128))
                firsts[j] = jnp.where(at == f, row, firsts[j])

    def flat(rows, width, copies=1):
        pieces = []
        count = min(16, 128 // width)
        for group in range(16 // count):
            total = jnp.zeros((1, 128), F32)
            for i in range(count):
                source = group * count + i
                row = jnp.where(lane[:1] < width, rows[source : source + 1], 0.0)
                for again in range(copies):
                    shift = i * width + 64 * again
                    total += pltpu.roll(row, shift, 1) if shift else row
            pieces.append(total)
        return jnp.concatenate(pieces, axis=1) if len(pieces) > 1 else pieces[0]

    w_out[512:528] = jnp.concatenate(
        [flat(firsts[0], 16), flat(firsts[1], 16), jnp.zeros((14, 256), F32)], axis=0
    ).astype(BF)
    w_in[2048:2064] = jnp.concatenate(
        [flat(firsts[2], 4, 2), flat(firsts[3], 4, 2), jnp.zeros((14, 128), F32)], axis=0
    ).astype(BF)
    s_up[...] = flat(firsts[4] + firsts[5], 64)


def piece_refs(refs):
    return list(refs[:4]) + [refs[4].at[k] for k in range(4)]


def pool_kernel(*refs):
    pieces, (w_own, w_other, pool_w, out, mine, padded, w_in) = piece_refs(refs), refs[5:]
    x, c, whose = lax.axis_index("x"), lax.axis_index("c"), owners()
    first = pl.ds(pl.multiple_of(c * 512, 512), 512)

    @pl.when(c == 0)
    def _():
        w_in[:, :64] = w_own[:, :64]
        w_in[:, 64:] = w_other[:, 64:]

    @pl.when(c == 1)
    def _():
        w_in[:, :64] = w_other[:, :64]
        w_in[:, 64:] = w_own[:, 64:]

    tail = w_in[2048:2064].astype(F32)
    s_in = tail[0:1] + tail[1:2]
    padded[0:128] = jnp.zeros((128, 128), BF)
    padded[128 + SEQ :] = jnp.zeros((128, 128), BF)

    @pl.loop(0, 4)
    def _(block):
        rows = pl.ds(pl.multiple_of(block * 256, 256), 256)
        total = jnp.zeros((256, 128), F32)
        squares = jnp.zeros((256, 128), F32)
        for k, piece in enumerate(pieces):
            values = piece[rows, :]
            total += dot(values, w_in[pl.ds(pl.multiple_of(whose[k] * 256, 256), 256), :])
            wide = values.astype(F32)
            wide = wide * wide
            squares += wide[:, :128] + wide[:, 128:]
        scale = lax.rsqrt(jnp.sum(squares, axis=1, keepdims=True) / 2048 + EPS)
        padded[pl.ds(pl.multiple_of(128 + block * 256, 128), 256), :] = (total * scale * s_in).astype(BF)

    half = jnp.left_shift(1, x)
    row = lax.broadcasted_iota(jnp.int32, (256, 512), 0)
    source = lax.broadcasted_iota(jnp.int32, (256, 512), 1) - 128
    band = jnp.where((source >= row - half) & (source < row + half), 1.0, 0.0).astype(BF)
    own = pool_w[x]

    @pl.loop(0, 4)
    def _(block):
        sums = dot(band, padded[pl.ds(pl.multiple_of(block * 256, 256), 512), :])
        at = lax.broadcasted_iota(jnp.int32, (256, 128), 0) + block * 256
        counts = jnp.minimum(at + half, SEQ) - jnp.maximum(at - half, 0)
        here = padded[pl.ds(pl.multiple_of(128 + block * 256, 128), 256), :].astype(F32)
        pooled = (sums / counts.astype(F32) - here).astype(BF)
        out[pl.ds(pl.multiple_of(block * 256, 256), 256), :] = dot(pooled, own).astype(BF)

    mine[...] = out[first, :]


def mix_kernel(*refs):
    pieces, grouped, near, across = piece_refs(refs), refs[5], refs[6:9], refs[9]
    weights = list(refs[10:14]) + [refs[14].at[k] for k in range(4)]
    mixed, own, factor = refs[15:]
    chips, whose = around(lax.axis_index("x")), owners()
    c = lax.axis_index("c")

    @pl.loop(0, 2)
    def _(block):
        rows = pl.ds(pl.multiple_of(block * 512, 512), 512)
        squares = jnp.zeros((512, 128), F32)
        left = jnp.concatenate(
            [grouped[rows, :]] + [jnp.where(block == c, a[...], across[k]) for k, a in enumerate(near)],
            axis=1,
        )
        for k in range(8):
            weight = jnp.concatenate(
                [weights[k][pl.ds(pl.multiple_of(chips[j] * 128, 128), 128), :] for j in range(4)],
                axis=0,
            )
            scale = weights[k][512:513, :].astype(F32) + weights[k][513:514, :].astype(F32)
            value = (pieces[k][rows, :].astype(F32) + dot(left, weight) * scale).astype(BF)
            mixed[rows, pl.ds(pl.multiple_of(whose[k] * 256, 256), 256)] = value
            if k == 0:
                own[rows, :] = value
            wide = value.astype(F32)
            wide = wide * wide
            squares += wide[:, :128] + wide[:, 128:]
        mean = jnp.sum(squares, axis=1, keepdims=True) / 2048
        factor[rows, :] = jnp.broadcast_to(lax.rsqrt(mean + EPS), (512, 128))


def up_kernel(mixed, factor, s_up, b0, b1, b2, b3, b4, hidden):
    ys, zs = around(lax.axis_index("y")), around(lax.axis_index("z"))
    parts = [b.at[pl.ds(2 * k, 2)] for b in (b0, b1, b2) for k in range(2)] + [b3, b4]

    @pl.loop(0, 8)
    def _(step):
        rows = pl.ds(pl.multiple_of(lax.rem(step, 2) * 512, 512), 512)
        cols = pl.ds(pl.multiple_of(lax.div(step, 2) * 256, 256), 256)
        total = jnp.zeros((512, 256), F32)
        for k in range(8):
            left = [
                mixed[rows, pl.ds(pl.multiple_of((4 * zs[k // 2] + ys[2 * (k % 2) + i]) * 128, 128), 128)]
                for i in range(2)
            ]
            total += dot(jnp.concatenate(left, axis=1), parts[k][:, :, cols].reshape(256, 256))
        scale = jnp.concatenate([factor[rows, :]] * 2, axis=1) * s_up[:, cols]
        value = jnp.maximum(total * scale, 0.0)
        hidden[rows, cols] = (value * value).astype(BF)


def down_kernel(steps, hidden, b0, b1, b2, b3, b4, own, other):
    x, y, z = (lax.axis_index(name) for name in ("x", "y", "z"))
    core = lax.shift_right_logical(y, 1)
    y_is_own = core == lax.axis_index("c")
    low_is_own = y_is_own == (jnp.bitwise_and(y, 1) == 1)
    side = jnp.bitwise_and(y, 1)

    @pl.loop(0, 2 * len(steps))
    def _(step):
        rows = pl.ds(pl.multiple_of(lax.rem(step, 2) * 512, 512), 512)
        k = lax.div(step, 2)
        chip = lax.rem(x + ((2 * k + 1) if len(steps) > 1 else steps[0]), 4)
        away = lax.rem(chip - z + 4, 4)
        place = jnp.where(away == 0, 0, jnp.where(away == 1, 2, jnp.where(away == 2, 3, 1)))
        inner = jnp.bitwise_and(place, 1)
        far = jnp.where(place < 2, b3[inner], b4[inner])
        for first, second, first_is_own, lane in (
            (b0[place], far, y_is_own, side),
            (b1[place], b2[place], low_is_own, 1 - side),
        ):
            weight = jnp.concatenate(
                [jnp.where(first_is_own, second, first), jnp.where(first_is_own, first, second)], axis=0
            )
            value = dot_t(hidden[rows, :], weight).astype(BF)
            lanes = pl.ds(pl.multiple_of(lane * 128, 128), 128)
            other[k, rows, lanes] = value[:, :128]
            own[k, rows, lanes] = value[:, 128:]


def along(bundle, axes):
    low, high = send(bundle, axes, 1), send(bundle, axes, -1)
    return [bundle, low, high, send(low[:2], axes, 1), send(high[2:], axes, -1)]


def three(array, axes):
    far = send(array, axes, 2)
    return [send(array, axes, 1), send(array, axes, -1), far]


def near_three(array):
    return three(array, "x")


def bf(*shape):
    return jax.ShapeDtypeStruct(shape, BF)


def f32(*shape):
    return jax.ShapeDtypeStruct(shape, F32)


def layer(
    stream, norm_gain, w_in, s_in, pool_w, w_out, s_out, ffn_gain, w_up, s_up, w_down, s_down
):
    ring_z = ("rep", "z")
    tokens = stream[0]

    near = near_three(tokens)
    pieces = [tokens] + near
    pieces.append(swapped(jnp.stack(pieces)))

    arrays = (
        norm_gain.reshape(16, 128),
        w_in.T,
        s_in[None],
        w_out,
        s_out[None],
        ffn_gain.reshape(16, 128),
        w_up,
        s_up[None],
        w_down,
        s_down[None],
    )
    packet, up, down = call(
        prep_kernel,
        (bf(24, 1024), bf(128, 1024), bf(128, 1024)),
        [pltpu.VMEM((24, 1024), F32)]
        + [pltpu.VMEM(a.shape, F32) for a in arrays]
        + [pltpu.SemaphoreType.DMA((10,))],
        60,
        1_000_000,
        *arrays,
        in_hbm=10,
    )
    mixer = jnp.stack([packet] + three(packet, ring_z))
    up_bundle = [up] + three(up, "y")
    down_bundle = [down] + three(down, ring_z)
    mixers = [mixer] + three(mixer, "y")
    up_parts = along(jnp.stack(up_bundle), ring_z)
    down_parts = along(jnp.stack(down_bundle), "y")
    w_in_own, out_own, s_up_row = call(
        unpack_kernel, (bf(2064, 128), bf(528, 256), f32(1, 1024)), [], 8, 1_000_000, *mixers
    )

    w_in_other = swapped(w_in_own)
    grouped, mine = call(
        pool_kernel,
        (bf(SEQ, 128), bf(512, 128)),
        [pltpu.VMEM((SEQ + 256, 128), BF), pltpu.VMEM((2064, 128), BF)],
        16,
        800_000_000,
        *pieces,
        w_in_own,
        w_in_other,
        pool_w,
    )
    near = near_three(mine)
    across = swapped(jnp.stack(near))
    outs = [out_own] + near_three(out_own)
    outs.append(swapped(jnp.stack(outs)))
    mixed, mixed_own, factor = call(
        mix_kernel,
        (bf(SEQ, 2048), bf(SEQ, 256), f32(SEQ, 128)),
        [],
        32,
        2_200_000_000,
        *pieces,
        grouped,
        *near,
        across,
        *outs,
    )

    hidden = call(
        up_kernel, bf(SEQ, 1024), [], 32, 4_300_000_000, mixed, factor, s_up_row, *up_parts
    )

    def block_sums(steps):
        count = len(steps)
        own, other = call(
            functools.partial(down_kernel, steps),
            (bf(count, SEQ, 256), bf(count, SEQ, 256)),
            [],
            32,
            1_075_000_000 * count,
            hidden,
            *down_parts,
        )
        crossed = swapped(other)
        return [own[k].astype(F32) + crossed[k].astype(F32) for k in range(count)]

    (far,) = block_sums((2,))
    from_low, from_high = send(far[:512].astype(BF), "x", 1), send(far[512:].astype(BF), "x", -1)
    after, before = block_sums((1, 3))
    (here,) = block_sums((0,))
    after = jnp.concatenate([after[:512] + from_low.astype(F32), after[512:]], axis=0)
    before = jnp.concatenate([before[:512], before[512:] + from_high.astype(F32)], axis=0)
    low, high = send(after.astype(BF), "x", 1), send(before.astype(BF), "x", -1)
    total = mixed_own.astype(F32) + here + low.astype(F32) + high.astype(F32)
    return total.astype(BF)[None]


def solution(mesh):
    finer = Mesh(
        mesh.devices.reshape(mesh.shape["rep"], 4, 4, 4, 2),
        ("rep", "z", "y", "x", "c"),
    )
    rows = ("rep", "z", "y")
    both = ("x", "c", "z", "y")
    return jax.shard_map(
        layer,
        mesh=finer,
        in_specs=(
            P(rows, None, TP),
            P(),
            P(FS, TP),
            P(both),
            P(),
            P(FS, TP),
            P(both),
            P(),
            P(FS, TP),
            P(both),
            P(TP, FS),
            P(FS),
        ),
        out_specs=P(rows, None, TP),
        check_vma=False,
    )
```

```python
import functools

import jax
import jax.numpy as jnp
from jax import lax
from jax.experimental import pallas as pl
from jax.experimental.pallas import tpu as pltpu
from jax.sharding import Mesh
from jax.sharding import PartitionSpec as P


BF = jnp.bfloat16
F32 = jnp.float32
EPS = 0.25
SEQ = 1024
FS = ("z", "y")
TP = ("x", "c")
VMEM = pl.BlockSpec(memory_space=pltpu.VMEM)


def send(array, axes, shift):
    count = lax.axis_size(axes)
    return lax.ppermute(array, axes, [(i, (i + shift) % count) for i in range(count)])


def swapped(array):
    return send(array, "c", 1)


def two_parts(values):
    high = values.astype(BF).astype(F32)
    return high, values - high


def dot(a, b):
    return jnp.dot(a, b, preferred_element_type=F32)


def dot_t(a, b):
    return lax.dot_general(a, b, (((1,), (1,)), ((), ())), preferred_element_type=F32)


def around(at):
    return [at] + [lax.rem(at + step, 4) for step in (3, 1, 2)]


def owners():
    x, c = lax.axis_index("x"), lax.axis_index("c")
    return [2 * chip + c for chip in around(x)] + [2 * chip + 1 - c for chip in around(x)]


def call(kernel, out_shape, scratch, limit_mb, flops, *args, in_hbm=0):
    moved = sum(a.size * a.dtype.itemsize for a in args)
    return pl.pallas_call(
        kernel,
        out_shape=out_shape,
        in_specs=[VMEM] * (len(args) - in_hbm) + [pl.BlockSpec(memory_space=pltpu.HBM)] * in_hbm,
        out_specs=jax.tree.map(lambda _: VMEM, out_shape),
        scratch_shapes=scratch,
        compiler_params=pltpu.CompilerParams(vmem_limit_bytes=limit_mb << 20),
        cost_estimate=pl.CostEstimate(flops=flops, bytes_accessed=moved, transcendentals=0),
    )(*args)


def column_of(row):
    return jnp.broadcast_to(row, (128, 128)).T


def prep_kernel(
    norm_gain_at, w_in_at, s_in_at, w_out_at, s_out_at, ffn_gain_at, w_up_at, s_up_at, w_down_at, s_down_at,
    mixer, up, down, small, norm_gain, w_in, s_in, w_out, s_out, ffn_gain, w_up, s_up, w_down, s_down, done,
):
    sources = (norm_gain_at, w_in_at, s_in_at, w_out_at, s_out_at, s_up_at, ffn_gain_at, w_up_at, w_down_at, s_down_at)
    targets = (norm_gain, w_in, s_in, w_out, s_out, s_up, ffn_gain, w_up, w_down, s_down)
    copies = [pltpu.make_async_copy(a, b, done.at[k]) for k, (a, b) in enumerate(zip(sources, targets))]
    for copy in copies:
        copy.start()
    for copy in copies[:6]:
        copy.wait()
    f = 4 * lax.axis_index("z") + lax.axis_index("y")
    own = jnp.concatenate([w_in[...]] * 2, axis=0).T * column_of(norm_gain[pl.ds(f, 1), :])
    low_lanes = lax.broadcasted_iota(jnp.int32, (8, 128), 1) < 64
    for j in range(8):
        lanes = slice(j * 128, j * 128 + 128)
        small[0:8, lanes] = jnp.where(low_lanes, own[j * 16 : j * 16 + 8], own[j * 16 + 8 : j * 16 + 16])
    for j in range(4):
        small[8:16, j * 256 : j * 256 + 256] = w_out[j * 8 : j * 8 + 8, :]
    small[16:24] = jnp.zeros((8, 1024), F32)
    for row, at in ((s_out[...], 0), (s_in[...], 256), (s_up[...], 512)):
        high, low = two_parts(row)
        small[16:17, at : at + row.shape[1]] = high
        small[16:17, at + 128 : at + 128 + row.shape[1]] = low
    mixer[...] = small[...].astype(BF)
    for copy in copies[6:]:
        copy.wait()
    gain = column_of(ffn_gain[pl.ds(f, 1), :])
    for j in range(8):
        lanes = slice(j * 128, j * 128 + 128)
        up[:, lanes] = (w_up[:, lanes] * gain).astype(BF)
        down[:, lanes] = (w_down[lanes, :] * s_down[...]).T.astype(BF)


def unpack_kernel(m0, m1, m2, m3, w_in, w_out, s_up):
    ys, zs = around(lax.axis_index("y")), around(lax.axis_index("z"))
    lane = lax.broadcasted_iota(jnp.int32, (16, 128), 1)
    at = lax.broadcasted_iota(jnp.int32, (16, 128), 0)
    low_lanes = lane[:8] < 64
    firsts = [jnp.zeros((16, 128), F32) for _ in range(6)]
    for m, yy in zip((m0, m1, m2, m3), ys):
        for k, zz in enumerate(zs):
            f = 4 * zz + yy
            block = m[k].astype(F32)
            for j in range(8):
                part = block[:8, j * 128 : j * 128 + 128]
                turned = pltpu.roll(part, 64, 1)
                rows = jnp.concatenate(
                    [jnp.where(low_lanes, part, turned), jnp.where(low_lanes, turned, part)], axis=0
                )
                w_in[pl.ds(pl.multiple_of(f * 128 + j * 16, 16), 16), :] = rows.astype(BF)
            rows = jnp.concatenate([block[8:16, j * 256 : j * 256 + 256] for j in range(4)], axis=0)
            w_out[pl.ds(pl.multiple_of(f * 32, 32), 32), :] = rows.astype(BF)
            for j in range(6):
                row = jnp.broadcast_to(block[16:17, j * 128 : j * 128 + 128], (16, 128))
                firsts[j] = jnp.where(at == f, row, firsts[j])

    def flat(rows, width, copies=1):
        pieces = []
        count = min(16, 128 // width)
        for group in range(16 // count):
            total = jnp.zeros((1, 128), F32)
            for i in range(count):
                source = group * count + i
                row = jnp.where(lane[:1] < width, rows[source : source + 1], 0.0)
                for again in range(copies):
                    shift = i * width + 64 * again
                    total += pltpu.roll(row, shift, 1) if shift else row
            pieces.append(total)
        return jnp.concatenate(pieces, axis=1) if len(pieces) > 1 else pieces[0]

    w_out[512:528] = jnp.concatenate(
        [flat(firsts[0], 16), flat(firsts[1], 16), jnp.zeros((14, 256), F32)], axis=0
    ).astype(BF)
    w_in[2048:2064] = jnp.concatenate(
        [flat(firsts[2], 4, 2), flat(firsts[3], 4, 2), jnp.zeros((14, 128), F32)], axis=0
    ).astype(BF)
    s_up[...] = flat(firsts[4] + firsts[5], 64)


def piece_refs(refs):
    return list(refs[:4]) + [refs[4].at[k] for k in range(4)]


def pool_kernel(*refs):
    pieces, (w_own, w_other, pool_w, out, mine, padded, w_in) = piece_refs(refs), refs[5:]
    x, c, whose = lax.axis_index("x"), lax.axis_index("c"), owners()
    first = pl.ds(pl.multiple_of(c * 512, 512), 512)

    @pl.when(c == 0)
    def _():
        w_in[:, :64] = w_own[:, :64]
        w_in[:, 64:] = w_other[:, 64:]

    @pl.when(c == 1)
    def _():
        w_in[:, :64] = w_other[:, :64]
        w_in[:, 64:] = w_own[:, 64:]

    tail = w_in[2048:2064].astype(F32)
    s_in = tail[0:1] + tail[1:2]
    padded[0:128] = jnp.zeros((128, 128), BF)
    padded[128 + SEQ :] = jnp.zeros((128, 128), BF)

    @pl.loop(0, 4)
    def _(block):
        rows = pl.ds(pl.multiple_of(block * 256, 256), 256)
        total = jnp.zeros((256, 128), F32)
        squares = jnp.zeros((256, 128), F32)
        for k, piece in enumerate(pieces):
            values = piece[rows, :]
            total += dot(values, w_in[pl.ds(pl.multiple_of(whose[k] * 256, 256), 256), :])
            wide = values.astype(F32)
            wide = wide * wide
            squares += wide[:, :128] + wide[:, 128:]
        scale = lax.rsqrt(jnp.sum(squares, axis=1, keepdims=True) / 2048 + EPS)
        padded[pl.ds(pl.multiple_of(128 + block * 256, 128), 256), :] = (total * scale * s_in).astype(BF)

    half = jnp.left_shift(1, x)
    row = lax.broadcasted_iota(jnp.int32, (256, 512), 0)
    source = lax.broadcasted_iota(jnp.int32, (256, 512), 1) - 128
    band = jnp.where((source >= row - half) & (source < row + half), 1.0, 0.0).astype(BF)
    own = pool_w[x]

    @pl.loop(0, 4)
    def _(block):
        sums = dot(band, padded[pl.ds(pl.multiple_of(block * 256, 256), 512), :])
        at = lax.broadcasted_iota(jnp.int32, (256, 128), 0) + block * 256
        counts = jnp.minimum(at + half, SEQ) - jnp.maximum(at - half, 0)
        here = padded[pl.ds(pl.multiple_of(128 + block * 256, 128), 256), :].astype(F32)
        pooled = (sums / counts.astype(F32) - here).astype(BF)
        out[pl.ds(pl.multiple_of(block * 256, 256), 256), :] = dot(pooled, own).astype(BF)

    mine[...] = out[first, :]


def mix_kernel(*refs):
    pieces, grouped, near, across = piece_refs(refs), refs[5], refs[6:9], refs[9]
    weights = list(refs[10:14]) + [refs[14].at[k] for k in range(4)]
    mixed, own, factor = refs[15:]
    chips, whose = around(lax.axis_index("x")), owners()
    c = lax.axis_index("c")

    @pl.loop(0, 4)
    def _(block):
        rows = pl.ds(pl.multiple_of(block * 256, 256), 256)
        inner = pl.ds(pl.multiple_of(lax.rem(block, 2) * 256, 256), 256)
        squares = jnp.zeros((256, 128), F32)
        left = jnp.concatenate(
            [grouped[rows, :]] + [
                jnp.where(lax.div(block, 2) == c, a[inner, :], across[k, inner, :])
                for k, a in enumerate(near)
            ],
            axis=1,
        )
        for k in range(8):
            weight = jnp.concatenate(
                [weights[k][pl.ds(pl.multiple_of(chips[j] * 128, 128), 128), :] for j in range(4)],
                axis=0,
            )
            scale = weights[k][512:513, :].astype(F32) + weights[k][513:514, :].astype(F32)
            value = (pieces[k][rows, :].astype(F32) + dot(left, weight) * scale).astype(BF)
            mixed[rows, pl.ds(pl.multiple_of(whose[k] * 256, 256), 256)] = value
            if k == 0:
                own[rows, :] = value
            wide = value.astype(F32)
            wide = wide * wide
            squares += wide[:, :128] + wide[:, 128:]
        mean = jnp.sum(squares, axis=1, keepdims=True) / 2048
        factor[rows, :] = jnp.broadcast_to(lax.rsqrt(mean + EPS), (256, 128))


def up_parts_sum(mixed, parts, zs, rows, cols, total):
    ys = around(lax.axis_index("y"))
    for k, part in enumerate(parts):
        left = [
            mixed[rows, pl.ds(pl.multiple_of((4 * zs[k // 2] + ys[2 * (k % 2) + i]) * 128, 128), 128)]
            for i in range(2)
        ]
        total += dot(jnp.concatenate(left, axis=1), part[:, :, cols].reshape(256, 256))
    return total


def tile_of(step):
    rows = pl.ds(pl.multiple_of(lax.rem(step, 2) * 512, 512), 512)
    return rows, pl.ds(pl.multiple_of(lax.div(step, 2) * 256, 256), 256)


def up_near_kernel(mixed, *refs):
    parts, out = refs[:-1], refs[-1]
    zs = around(lax.axis_index("z"))
    if len(parts) == 3:
        parts = [b.at[pl.ds(2 * k, 2)] for b in parts for k in range(2)]

    @pl.loop(0, 4 * 2)
    def _(step):
        rows, cols = tile_of(step)
        out[rows, cols] = up_parts_sum(mixed, parts, zs, rows, cols, jnp.zeros((512, 256), F32))


def up_far_kernel(mixed, factor, s_up, near, b3, b4, hidden):
    zs = around(lax.axis_index("z"))[3:]

    @pl.loop(0, 4 * 2)
    def _(step):
        rows, cols = tile_of(step)
        total = up_parts_sum(mixed, (b3, b4), zs, rows, cols, near[rows, cols])
        scale = jnp.concatenate([factor[rows, :]] * 2, axis=1) * s_up[:, cols]
        value = jnp.maximum(total * scale, 0.0)
        hidden[rows, cols] = (value * value).astype(BF)


def down_kernel(steps, hidden, b0, b1, b2, b3, b4, own, other):
    x, y, z = (lax.axis_index(name) for name in ("x", "y", "z"))
    core = lax.shift_right_logical(y, 1)
    y_is_own = core == lax.axis_index("c")
    low_is_own = y_is_own == (jnp.bitwise_and(y, 1) == 1)
    side = jnp.bitwise_and(y, 1)

    @pl.loop(0, 4 * len(steps))
    def _(step):
        rows = pl.ds(pl.multiple_of(lax.rem(step, 4) * 256, 256), 256)
        k = lax.div(step, 4)
        chip = lax.rem(x + ((2 * k + 1) if len(steps) > 1 else steps[0]), 4)
        away = lax.rem(chip - z + 4, 4)
        place = jnp.where(away == 0, 0, jnp.where(away == 1, 2, jnp.where(away == 2, 3, 1)))
        inner = jnp.bitwise_and(place, 1)
        far = jnp.where(place < 2, b3[inner], b4[inner])
        for first, second, first_is_own, lane in (
            (b0[place], far, y_is_own, side),
            (b1[place], b2[place], low_is_own, 1 - side),
        ):
            weight = jnp.concatenate(
                [jnp.where(first_is_own, second, first), jnp.where(first_is_own, first, second)], axis=0
            )
            value = dot_t(hidden[rows, :], weight).astype(BF)
            lanes = pl.ds(pl.multiple_of(lane * 128, 128), 128)
            other[k, rows, lanes] = value[:, :128]
            own[k, rows, lanes] = value[:, 128:]


def along(bundle, axes):
    low, high = send(bundle, axes, 1), send(bundle, axes, -1)
    return [bundle, low, high, send(low[:2], axes, 1), send(high[2:], axes, -1)]


def three(array, axes):
    far = send(array, axes, 2)
    return [send(array, axes, 1), send(array, axes, -1), far]


def near_three(array):
    return three(array, "x")


def bf(*shape):
    return jax.ShapeDtypeStruct(shape, BF)


def f32(*shape):
    return jax.ShapeDtypeStruct(shape, F32)


def layer(
    stream, norm_gain, w_in, s_in, pool_w, w_out, s_out, ffn_gain, w_up, s_up, w_down, s_down
):
    ring_z = ("rep", "z")
    tokens = stream[0]

    near = near_three(tokens)
    pieces = [tokens] + near
    pieces.append(swapped(jnp.stack(pieces)))

    arrays = (
        norm_gain.reshape(16, 128),
        w_in.T,
        s_in[None],
        w_out,
        s_out[None],
        ffn_gain.reshape(16, 128),
        w_up,
        s_up[None],
        w_down,
        s_down[None],
    )
    packet, up, down = call(
        prep_kernel,
        (bf(24, 1024), bf(128, 1024), bf(128, 1024)),
        [pltpu.VMEM((24, 1024), F32)]
        + [pltpu.VMEM(a.shape, F32) for a in arrays]
        + [pltpu.SemaphoreType.DMA((10,))],
        60,
        1_000_000,
        *arrays,
        in_hbm=10,
    )
    mixer = jnp.stack([packet] + three(packet, ring_z))
    up_bundle = [up] + three(up, "y")
    down_bundle = [down] + three(down, ring_z)
    mixers = [mixer] + three(mixer, "y")
    up_parts = along(jnp.stack(up_bundle), ring_z)
    down_parts = along(jnp.stack(down_bundle), "y")
    w_in_own, out_own, s_up_row = call(
        unpack_kernel, (bf(2064, 128), bf(528, 256), f32(1, 1024)), [], 8, 1_000_000, *mixers
    )

    w_in_other = swapped(w_in_own)
    grouped, mine = call(
        pool_kernel,
        (bf(SEQ, 128), bf(512, 128)),
        [pltpu.VMEM((SEQ + 256, 128), BF), pltpu.VMEM((2064, 128), BF)],
        16,
        800_000_000,
        *pieces,
        w_in_own,
        w_in_other,
        pool_w,
    )
    near = near_three(mine)
    across = swapped(jnp.stack(near))
    outs = [out_own] + near_three(out_own)
    outs.append(swapped(jnp.stack(outs)))
    mixed, mixed_own, factor = call(
        mix_kernel,
        (bf(SEQ, 2048), bf(SEQ, 256), f32(SEQ, 128)),
        [],
        32,
        2_200_000_000,
        *pieces,
        grouped,
        *near,
        across,
        *outs,
    )

    sums = call(
        up_near_kernel, f32(SEQ, 1024), [], 24, 3_200_000_000, mixed, *up_parts[:-2]
    )
    hidden = call(up_far_kernel, bf(SEQ, 1024), [], 24, 1_100_000_000, mixed, factor, s_up_row, sums, *up_parts[-2:])

    def block_sums(steps):
        count = len(steps)
        own, other = call(
            functools.partial(down_kernel, steps),
            (bf(count, SEQ, 256), bf(count, SEQ, 256)),
            [],
            32,
            1_075_000_000 * count,
            hidden,
            *down_parts,
        )
        crossed = swapped(other)
        return [own[k].astype(F32) + crossed[k].astype(F32) for k in range(count)]

    (far,) = block_sums((2,))
    from_low, from_high = send(far[:512].astype(BF), "x", 1), send(far[512:].astype(BF), "x", -1)
    after, before = block_sums((1, 3))
    (here,) = block_sums((0,))
    after = jnp.concatenate([after[:512] + from_low.astype(F32), after[512:]], axis=0)
    before = jnp.concatenate([before[:512], before[512:] + from_high.astype(F32)], axis=0)
    low, high = send(after.astype(BF), "x", 1), send(before.astype(BF), "x", -1)
    total = mixed_own.astype(F32) + here + low.astype(F32) + high.astype(F32)
    return total.astype(BF)[None]


def solution(mesh):
    finer = Mesh(
        mesh.devices.reshape(mesh.shape["rep"], 4, 4, 4, 2),
        ("rep", "z", "y", "x", "c"),
    )
    rows = ("rep", "z", "y")
    both = ("x", "c", "z", "y")
    return jax.shard_map(
        layer,
        mesh=finer,
        in_specs=(
            P(rows, None, TP),
            P(),
            P(FS, TP),
            P(both),
            P(),
            P(FS, TP),
            P(both),
            P(),
            P(FS, TP),
            P(both),
            P(TP, FS),
            P(FS),
        ),
        out_specs=P(rows, None, TP),
        check_vma=False,
    )
```

```python
import functools

import jax
import jax.numpy as jnp
from jax import lax
from jax.experimental import pallas as pl
from jax.experimental.pallas import tpu as pltpu
from jax.sharding import Mesh
from jax.sharding import PartitionSpec as P


BF = jnp.bfloat16
F32 = jnp.float32
EPS = 0.25
SEQ = 1024
FS = ("z", "y")
TP = ("x", "c")
VMEM = pl.BlockSpec(memory_space=pltpu.VMEM)


def send(array, axes, shift):
    count = lax.axis_size(axes)
    return lax.ppermute(array, axes, [(i, (i + shift) % count) for i in range(count)])


def swapped(array):
    return send(array, "c", 1)


def two_parts(values):
    high = values.astype(BF).astype(F32)
    return high, values - high


def dot(a, b):
    return jnp.dot(a, b, preferred_element_type=F32)


def dot_t(a, b):
    return lax.dot_general(a, b, (((1,), (1,)), ((), ())), preferred_element_type=F32)


def around(at):
    return [at] + [lax.rem(at + step, 4) for step in (3, 1, 2)]


def owners():
    x, c = lax.axis_index("x"), lax.axis_index("c")
    return [2 * chip + c for chip in around(x)] + [2 * chip + 1 - c for chip in around(x)]


def call(kernel, out_shape, scratch, limit_mb, flops, *args, in_hbm=0):
    moved = sum(a.size * a.dtype.itemsize for a in args)
    return pl.pallas_call(
        kernel,
        out_shape=out_shape,
        in_specs=[VMEM] * (len(args) - in_hbm) + [pl.BlockSpec(memory_space=pltpu.HBM)] * in_hbm,
        out_specs=jax.tree.map(lambda _: VMEM, out_shape),
        scratch_shapes=scratch,
        compiler_params=pltpu.CompilerParams(vmem_limit_bytes=limit_mb << 20),
        cost_estimate=pl.CostEstimate(flops=flops, bytes_accessed=moved, transcendentals=0),
    )(*args)


def column_of(row):
    return jnp.broadcast_to(row, (128, 128)).T


def prep_kernel(
    norm_gain_at, w_in_at, s_in_at, w_out_at, s_out_at, ffn_gain_at, w_up_at, s_up_at, w_down_at, s_down_at,
    packet, up, top, bottom, small, norm_gain, w_in, s_in, w_out, s_out, ffn_gain, w_up, s_up, w_down, s_down, done,
):
    sources = (norm_gain_at, w_in_at, s_in_at, w_out_at, s_out_at, s_up_at, ffn_gain_at, w_up_at, w_down_at, s_down_at)
    targets = (norm_gain, w_in, s_in, w_out, s_out, s_up, ffn_gain, w_up, w_down, s_down)
    copies = [pltpu.make_async_copy(a, b, done.at[k]) for k, (a, b) in enumerate(zip(sources, targets))]
    for copy in copies:
        copy.start()
    for copy in copies[:6]:
        copy.wait()
    f = 4 * lax.axis_index("z") + lax.axis_index("y")
    own = jnp.concatenate([w_in[...]] * 2, axis=0).T * column_of(norm_gain[pl.ds(f, 1), :])
    low_lanes = lax.broadcasted_iota(jnp.int32, (8, 128), 1) < 64
    for j in range(8):
        lanes = slice(j * 128, j * 128 + 128)
        small[0:8, lanes] = jnp.where(low_lanes, own[j * 16 : j * 16 + 8], own[j * 16 + 8 : j * 16 + 16])
    for j in range(4):
        small[8:16, j * 256 : j * 256 + 256] = w_out[j * 8 : j * 8 + 8, :]
    small[16:24] = jnp.zeros((8, 1024), F32)
    for row, at in ((s_out[...], 0), (s_in[...], 256), (s_up[...], 512)):
        high, low = two_parts(row)
        small[16:17, at : at + row.shape[1]] = high
        small[16:17, at + 128 : at + 128 + row.shape[1]] = low
    packet[128:] = small[...].astype(BF)
    for copy in copies[6:]:
        copy.wait()
    gain = column_of(ffn_gain[pl.ds(f, 1), :])
    for j in range(8):
        lanes = slice(j * 128, j * 128 + 128)
        up[:, lanes] = (w_up[:, lanes] * gain).astype(BF)
        packet[:128, lanes] = (w_down[lanes, :] * s_down[...]).T.astype(BF)
    top[...] = up[:64]
    bottom[...] = up[64:]


def unpack_kernel(m0, m1, m2, m3, m4, w_in, w_out, s_up):
    ys, zs = around(lax.axis_index("y")), around(lax.axis_index("z"))
    lane = lax.broadcasted_iota(jnp.int32, (16, 128), 1)
    at = lax.broadcasted_iota(jnp.int32, (16, 128), 0)
    low_lanes = lane[:8] < 64
    firsts = [jnp.zeros((16, 128), F32) for _ in range(6)]
    for p, zz in enumerate(zs):
        for k, yy in enumerate(ys):
            f = 4 * zz + yy
            source = (m0, m1, m2)[p].at[k] if p < 3 else (m3, m4)[k // 2].at[k % 2]
            block = source[...].astype(F32)
            for j in range(8):
                part = block[:8, j * 128 : j * 128 + 128]
                turned = pltpu.roll(part, 64, 1)
                rows = jnp.concatenate(
                    [jnp.where(low_lanes, part, turned), jnp.where(low_lanes, turned, part)], axis=0
                )
                w_in[pl.ds(pl.multiple_of(f * 128 + j * 16, 16), 16), :] = rows.astype(BF)
            rows = jnp.concatenate([block[8:16, j * 256 : j * 256 + 256] for j in range(4)], axis=0)
            w_out[pl.ds(pl.multiple_of(f * 32, 32), 32), :] = rows.astype(BF)
            for j in range(6):
                row = jnp.broadcast_to(block[16:17, j * 128 : j * 128 + 128], (16, 128))
                firsts[j] = jnp.where(at == f, row, firsts[j])

    def flat(rows, width, copies=1):
        pieces = []
        count = min(16, 128 // width)
        for group in range(16 // count):
            total = jnp.zeros((1, 128), F32)
            for i in range(count):
                source = group * count + i
                row = jnp.where(lane[:1] < width, rows[source : source + 1], 0.0)
                for again in range(copies):
                    shift = i * width + 64 * again
                    total += pltpu.roll(row, shift, 1) if shift else row
            pieces.append(total)
        return jnp.concatenate(pieces, axis=1) if len(pieces) > 1 else pieces[0]

    w_out[512:528] = jnp.concatenate(
        [flat(firsts[0], 16), flat(firsts[1], 16), jnp.zeros((14, 256), F32)], axis=0
    ).astype(BF)
    w_in[2048:2064] = jnp.concatenate(
        [flat(firsts[2], 4, 2), flat(firsts[3], 4, 2), jnp.zeros((14, 128), F32)], axis=0
    ).astype(BF)
    s_up[...] = flat(firsts[4] + firsts[5], 64)


def piece_refs(refs):
    return list(refs[:4]) + [refs[4].at[k] for k in range(4)]


def pool_kernel(*refs):
    pieces, (w_own, w_other, pool_w, out, mine, padded, w_in) = piece_refs(refs), refs[5:]
    x, c, whose = lax.axis_index("x"), lax.axis_index("c"), owners()
    first = pl.ds(pl.multiple_of(c * 512, 512), 512)

    @pl.when(c == 0)
    def _():
        w_in[:, :64] = w_own[:, :64]
        w_in[:, 64:] = w_other[:, 64:]

    @pl.when(c == 1)
    def _():
        w_in[:, :64] = w_other[:, :64]
        w_in[:, 64:] = w_own[:, 64:]

    tail = w_in[2048:2064].astype(F32)
    s_in = tail[0:1] + tail[1:2]
    padded[0:128] = jnp.zeros((128, 128), BF)
    padded[128 + SEQ :] = jnp.zeros((128, 128), BF)

    @pl.loop(0, 4)
    def _(block):
        rows = pl.ds(pl.multiple_of(block * 256, 256), 256)
        total = jnp.zeros((256, 128), F32)
        squares = jnp.zeros((256, 128), F32)
        for k, piece in enumerate(pieces):
            values = piece[rows, :]
            total += dot(values, w_in[pl.ds(pl.multiple_of(whose[k] * 256, 256), 256), :])
            wide = values.astype(F32)
            wide = wide * wide
            squares += wide[:, :128] + wide[:, 128:]
        scale = lax.rsqrt(jnp.sum(squares, axis=1, keepdims=True) / 2048 + EPS)
        padded[pl.ds(pl.multiple_of(128 + block * 256, 128), 256), :] = (total * scale * s_in).astype(BF)

    half = jnp.left_shift(1, x)
    row = lax.broadcasted_iota(jnp.int32, (256, 512), 0)
    source = lax.broadcasted_iota(jnp.int32, (256, 512), 1) - 128
    band = jnp.where((source >= row - half) & (source < row + half), 1.0, 0.0).astype(BF)
    own = pool_w[x]

    @pl.loop(0, 4)
    def _(block):
        sums = dot(band, padded[pl.ds(pl.multiple_of(block * 256, 256), 512), :])
        at = lax.broadcasted_iota(jnp.int32, (256, 128), 0) + block * 256
        counts = jnp.minimum(at + half, SEQ) - jnp.maximum(at - half, 0)
        here = padded[pl.ds(pl.multiple_of(128 + block * 256, 128), 256), :].astype(F32)
        pooled = (sums / counts.astype(F32) - here).astype(BF)
        out[pl.ds(pl.multiple_of(block * 256, 256), 256), :] = dot(pooled, own).astype(BF)

    mine[...] = out[first, :]


def mix_kernel(*refs):
    pieces, grouped, near, across = piece_refs(refs), refs[5], refs[6:9], refs[9]
    weights = list(refs[10:14]) + [refs[14].at[k] for k in range(4)]
    mixed, own, factor = refs[15:]
    chips, whose = around(lax.axis_index("x")), owners()
    c = lax.axis_index("c")

    @pl.loop(0, 4)
    def _(block):
        rows = pl.ds(pl.multiple_of(block * 256, 256), 256)
        inner = pl.ds(pl.multiple_of(lax.rem(block, 2) * 256, 256), 256)
        squares = jnp.zeros((256, 128), F32)
        left = jnp.concatenate(
            [grouped[rows, :]] + [
                jnp.where(lax.div(block, 2) == c, a[inner, :], across[k, inner, :])
                for k, a in enumerate(near)
            ],
            axis=1,
        )
        for k in range(8):
            weight = jnp.concatenate(
                [weights[k][pl.ds(pl.multiple_of(chips[j] * 128, 128), 128), :] for j in range(4)],
                axis=0,
            )
            scale = weights[k][512:513, :].astype(F32) + weights[k][513:514, :].astype(F32)
            value = (pieces[k][rows, :].astype(F32) + dot(left, weight) * scale).astype(BF)
            mixed[rows, pl.ds(pl.multiple_of(whose[k] * 256, 256), 256)] = value
            if k == 0:
                own[rows, :] = value
            wide = value.astype(F32)
            wide = wide * wide
            squares += wide[:, :128] + wide[:, 128:]
        mean = jnp.sum(squares, axis=1, keepdims=True) / 2048
        factor[rows, :] = jnp.broadcast_to(lax.rsqrt(mean + EPS), (256, 128))


def up_parts_sum(mixed, parts, ys, rows, cols, total):
    zs = around(lax.axis_index("z"))
    for k, part in enumerate(parts):
        left = [
            mixed[rows, pl.ds(pl.multiple_of((4 * zs[2 * (k % 2) + i] + ys[k // 2]) * 128, 128), 128)]
            for i in range(2)
        ]
        total += dot(jnp.concatenate(left, axis=1), part[:, :, cols].reshape(256, 256))
    return total


def tile_of(step):
    rows = pl.ds(pl.multiple_of(lax.rem(step, 2) * 512, 512), 512)
    return rows, pl.ds(pl.multiple_of(lax.div(step, 2) * 256, 256), 256)


def up_near_kernel(mixed, *refs):
    parts, out = refs[:-1], refs[-1]
    ys = around(lax.axis_index("y"))
    if len(parts) == 3:
        parts = [b.at[pl.ds(2 * k, 2)] for b in parts for k in range(2)]

    @pl.loop(0, 4 * 2)
    def _(step):
        rows, cols = tile_of(step)
        out[rows, cols] = up_parts_sum(mixed, parts, ys, rows, cols, jnp.zeros((512, 256), F32))


def up_far_kernel(mixed, factor, s_up, near, b3, b4, hidden):
    ys = around(lax.axis_index("y"))[3:]

    @pl.loop(0, 4 * 2)
    def _(step):
        rows, cols = tile_of(step)
        total = up_parts_sum(mixed, (b3, b4), ys, rows, cols, near[rows, cols])
        scale = jnp.concatenate([factor[rows, :]] * 2, axis=1) * s_up[:, cols]
        value = jnp.maximum(total * scale, 0.0)
        hidden[rows, cols] = (value * value).astype(BF)


def down_kernel(steps, hidden, b0, b1, b2, b3, b4, own, other, taken):
    x, y, z = (lax.axis_index(name) for name in ("x", "y", "z"))
    core = lax.shift_right_logical(y, 1)
    y_is_own = core == lax.axis_index("c")
    low_is_own = y_is_own == (jnp.bitwise_and(y, 1) == 1)
    side = jnp.bitwise_and(y, 1)

    @pl.loop(0, len(steps))
    def _(k):
        chip = lax.rem(x + ((2 * k + 1) if len(steps) > 1 else steps[0]), 4)
        away = lax.rem(chip - z + 4, 4)
        for place, source in ((0, b0), (3, b1), (1, b2)):

            @pl.when(away == place)
            def _(source=source):
                @pl.loop(0, 4)
                def _(i):
                    taken[i] = source[i]

        @pl.when(away == 2)
        def _():
            @pl.loop(0, 2)
            def _(i):
                taken[i] = b3[i]
                taken[i + 2] = b4[i]

        @pl.loop(0, 2)
        def _(block):
            rows = pl.ds(pl.multiple_of(block * 512, 512), 512)
            for first, second, first_is_own, lane in (
                (taken[0], taken[3], y_is_own, side),
                (taken[1], taken[2], low_is_own, 1 - side),
            ):
                weight = jnp.concatenate(
                    [jnp.where(first_is_own, second, first), jnp.where(first_is_own, first, second)],
                    axis=0,
                )
                value = dot_t(hidden[rows, :], weight).astype(BF)
                lanes = pl.ds(pl.multiple_of(lane * 128, 128), 128)
                other[k, rows, lanes] = value[:, :128]
                own[k, rows, lanes] = value[:, 128:]


def along(bundle, axes):
    low, high = send(bundle, axes, 1), send(bundle, axes, -1)
    return [bundle, low, high, send(low[:2], axes, 1), send(high[2:], axes, -1)]


def three(array, axes):
    far = send(array, axes, 2)
    return [send(array, axes, 1), send(array, axes, -1), far]


def near_three(array):
    return three(array, "x")


def bf(*shape):
    return jax.ShapeDtypeStruct(shape, BF)


def f32(*shape):
    return jax.ShapeDtypeStruct(shape, F32)


def layer(
    stream, norm_gain, w_in, s_in, pool_w, w_out, s_out, ffn_gain, w_up, s_up, w_down, s_down
):
    ring_z = ("rep", "z")
    tokens = stream[0]

    near = near_three(tokens)
    pieces = [tokens] + near
    pieces.append(swapped(jnp.stack(pieces)))

    arrays = (
        norm_gain.reshape(16, 128),
        w_in.T,
        s_in[None],
        w_out,
        s_out[None],
        ffn_gain.reshape(16, 128),
        w_up,
        s_up[None],
        w_down,
        s_down[None],
    )
    packet, up, top, bottom = call(
        prep_kernel,
        (bf(152, 1024), bf(128, 1024), bf(64, 1024), bf(64, 1024)),
        [pltpu.VMEM((24, 1024), F32)]
        + [pltpu.VMEM(a.shape, F32) for a in arrays]
        + [pltpu.SemaphoreType.DMA((10,))],
        60,
        1_000_000,
        *arrays,
        in_hbm=10,
    )
    packets = [packet] + three(packet, "y")
    far_top, far_bottom = send(top, ring_z, 2), send(bottom, ring_z, -2)
    low, high = send(up, ring_z, 1), send(up, ring_z, -1)
    far = jnp.concatenate([far_top, far_bottom], axis=0)
    up_bundle = jnp.stack([up, low, high, far])
    mixer = jnp.stack([p[128:] for p in packets])
    mixers = [mixer, send(mixer, ring_z, 1), send(mixer, ring_z, -1)]
    mixers += [send(mixer[:2], ring_z, 2), send(mixer[2:], ring_z, -2)]
    up_parts = along(up_bundle, "y")
    down_parts = along(jnp.stack([p[:128] for p in packets]), ring_z)
    w_in_own, out_own, s_up_row = call(
        unpack_kernel, (bf(2064, 128), bf(528, 256), f32(1, 1024)), [], 8, 1_000_000, *mixers
    )

    w_in_other = swapped(w_in_own)
    grouped, mine = call(
        pool_kernel,
        (bf(SEQ, 128), bf(512, 128)),
        [pltpu.VMEM((SEQ + 256, 128), BF), pltpu.VMEM((2064, 128), BF)],
        16,
        800_000_000,
        *pieces,
        w_in_own,
        w_in_other,
        pool_w,
    )
    near = near_three(mine)
    across = swapped(jnp.stack(near))
    outs = [out_own] + near_three(out_own)
    outs.append(swapped(jnp.stack(outs)))
    mixed, mixed_own, factor = call(
        mix_kernel,
        (bf(SEQ, 2048), bf(SEQ, 256), f32(SEQ, 128)),
        [],
        32,
        2_200_000_000,
        *pieces,
        grouped,
        *near,
        across,
        *outs,
    )

    sums = call(
        up_near_kernel, f32(SEQ, 1024), [], 24, 3_200_000_000, mixed, *up_parts[:-2]
    )
    hidden = call(up_far_kernel, bf(SEQ, 1024), [], 24, 1_100_000_000, mixed, factor, s_up_row, sums, *up_parts[-2:])

    def block_sums(steps):
        count = len(steps)
        own, other = call(
            functools.partial(down_kernel, steps),
            (bf(count, SEQ, 256), bf(count, SEQ, 256)),
            [pltpu.VMEM((4, 128, 1024), BF)],
            32,
            1_075_000_000 * count,
            hidden,
            *down_parts,
        )
        crossed = swapped(other)
        return [own[k].astype(F32) + crossed[k].astype(F32) for k in range(count)]

    (far,) = block_sums((2,))
    from_low = send(far[:512].astype(BF), "x", 1)
    from_high = send(far[512:].astype(BF), "x", -1)
    after, before = block_sums((1, 3))
    (here,) = block_sums((0,))
    after = jnp.concatenate([after[:512] + from_low.astype(F32), after[512:]], axis=0)
    before = jnp.concatenate([before[:512], before[512:] + from_high.astype(F32)], axis=0)
    low = send(after.astype(BF), "x", 1)
    high = send(before.astype(BF), "x", -1)
    total = mixed_own.astype(F32) + here + low.astype(F32) + high.astype(F32)
    return total.astype(BF)[None]


def solution(mesh):
    finer = Mesh(
        mesh.devices.reshape(mesh.shape["rep"], 4, 4, 4, 2),
        ("rep", "z", "y", "x", "c"),
    )
    rows = ("rep", "z", "y")
    both = ("x", "c", "z", "y")
    return jax.shard_map(
        layer,
        mesh=finer,
        in_specs=(
            P(rows, None, TP),
            P(),
            P(FS, TP),
            P(both),
            P(),
            P(FS, TP),
            P(both),
            P(),
            P(FS, TP),
            P(both),
            P(TP, FS),
            P(FS),
        ),
        out_specs=P(rows, None, TP),
        check_vma=False,
    )
```

```python
import functools

import jax
import jax.numpy as jnp
from jax import lax
from jax.experimental import pallas as pl
from jax.experimental.pallas import tpu as pltpu
from jax.sharding import Mesh
from jax.sharding import PartitionSpec as P


BF = jnp.bfloat16
F32 = jnp.float32
EPS = 0.25
SEQ = 1024
FS = ("z", "y")
TP = ("x", "c")
VMEM = pl.BlockSpec(memory_space=pltpu.VMEM)


def send(array, axes, shift):
    count = lax.axis_size(axes)
    return lax.ppermute(array, axes, [(i, (i + shift) % count) for i in range(count)])


def swapped(array):
    return send(array, "c", 1)


def two_parts(values):
    high = values.astype(BF).astype(F32)
    return high, values - high


def dot(a, b):
    return jnp.dot(a, b, preferred_element_type=F32)


def dot_t(a, b):
    return lax.dot_general(a, b, (((1,), (1,)), ((), ())), preferred_element_type=F32)


def around(at):
    return [at] + [lax.rem(at + step, 4) for step in (3, 1, 2)]


def owners():
    x, c = lax.axis_index("x"), lax.axis_index("c")
    return [2 * chip + c for chip in around(x)] + [2 * chip + 1 - c for chip in around(x)]


def call(kernel, out_shape, scratch, limit_mb, flops, *args, in_hbm=0):
    moved = sum(a.size * a.dtype.itemsize for a in args)
    return pl.pallas_call(
        kernel,
        out_shape=out_shape,
        in_specs=[VMEM] * (len(args) - in_hbm) + [pl.BlockSpec(memory_space=pltpu.HBM)] * in_hbm,
        out_specs=jax.tree.map(lambda _: VMEM, out_shape),
        scratch_shapes=scratch,
        compiler_params=pltpu.CompilerParams(vmem_limit_bytes=limit_mb << 20),
        cost_estimate=pl.CostEstimate(flops=flops, bytes_accessed=moved, transcendentals=0),
    )(*args)


def column_of(row):
    return jnp.broadcast_to(row, (128, 128)).T


def prep_kernel(
    norm_gain_at, w_in_at, s_in_at, w_out_at, s_out_at, ffn_gain_at, w_up_at, s_up_at, w_down_at, s_down_at,
    packet, up, top, bottom, small, norm_gain, w_in, s_in, w_out, s_out, ffn_gain, w_up, s_up, w_down, s_down, done,
):
    sources = (norm_gain_at, w_in_at, s_in_at, w_out_at, s_out_at, s_up_at, ffn_gain_at, w_up_at, w_down_at, s_down_at)
    targets = (norm_gain, w_in, s_in, w_out, s_out, s_up, ffn_gain, w_up, w_down, s_down)
    copies = [pltpu.make_async_copy(a, b, done.at[k]) for k, (a, b) in enumerate(zip(sources, targets))]
    for copy in copies:
        copy.start()
    for copy in copies[:6]:
        copy.wait()
    f = 4 * lax.axis_index("z") + lax.axis_index("y")
    own = jnp.concatenate([w_in[...]] * 2, axis=0).T * column_of(norm_gain[pl.ds(f, 1), :])
    low_lanes = lax.broadcasted_iota(jnp.int32, (8, 128), 1) < 64
    for j in range(8):
        lanes = slice(j * 128, j * 128 + 128)
        small[0:8, lanes] = jnp.where(low_lanes, own[j * 16 : j * 16 + 8], own[j * 16 + 8 : j * 16 + 16])
    for j in range(4):
        small[8:16, j * 256 : j * 256 + 256] = w_out[j * 8 : j * 8 + 8, :]
    small[16:24] = jnp.zeros((8, 1024), F32)
    for row, at in ((s_out[...], 0), (s_in[...], 256), (s_up[...], 512)):
        high, low = two_parts(row)
        small[16:17, at : at + row.shape[1]] = high
        small[16:17, at + 128 : at + 128 + row.shape[1]] = low
    packet[128:] = small[...].astype(BF)
    for copy in copies[6:]:
        copy.wait()
    gain = column_of(ffn_gain[pl.ds(f, 1), :])
    for j in range(8):
        lanes = slice(j * 128, j * 128 + 128)
        up[:, lanes] = (w_up[:, lanes] * gain).astype(BF)
        packet[:128, lanes] = (w_down[lanes, :] * s_down[...]).T.astype(BF)
    top[...] = up[:64]
    bottom[...] = up[64:]


def unpack_kernel(m0, m1, m2, m3, m4, w_in, w_out, s_up):
    ys, zs = around(lax.axis_index("y")), around(lax.axis_index("z"))
    lane = lax.broadcasted_iota(jnp.int32, (16, 128), 1)
    at = lax.broadcasted_iota(jnp.int32, (16, 128), 0)
    low_lanes = lane[:8] < 64
    firsts = [jnp.zeros((16, 128), F32) for _ in range(6)]
    for p, zz in enumerate(zs):
        for k, yy in enumerate(ys):
            f = 4 * zz + yy
            source = (m0, m1, m2)[p].at[k] if p < 3 else (m3, m4)[k // 2].at[k % 2]
            block = source[...].astype(F32)
            for j in range(8):
                part = block[:8, j * 128 : j * 128 + 128]
                turned = pltpu.roll(part, 64, 1)
                rows = jnp.concatenate(
                    [jnp.where(low_lanes, part, turned), jnp.where(low_lanes, turned, part)], axis=0
                )
                w_in[pl.ds(pl.multiple_of(f * 128 + j * 16, 16), 16), :] = rows.astype(BF)
            rows = jnp.concatenate([block[8:16, j * 256 : j * 256 + 256] for j in range(4)], axis=0)
            w_out[pl.ds(pl.multiple_of(f * 32, 32), 32), :] = rows.astype(BF)
            for j in range(6):
                row = jnp.broadcast_to(block[16:17, j * 128 : j * 128 + 128], (16, 128))
                firsts[j] = jnp.where(at == f, row, firsts[j])

    def flat(rows, width, copies=1):
        pieces = []
        count = min(16, 128 // width)
        for group in range(16 // count):
            total = jnp.zeros((1, 128), F32)
            for i in range(count):
                source = group * count + i
                row = jnp.where(lane[:1] < width, rows[source : source + 1], 0.0)
                for again in range(copies):
                    shift = i * width + 64 * again
                    total += pltpu.roll(row, shift, 1) if shift else row
            pieces.append(total)
        return jnp.concatenate(pieces, axis=1) if len(pieces) > 1 else pieces[0]

    w_out[512:528] = jnp.concatenate(
        [flat(firsts[0], 16), flat(firsts[1], 16), jnp.zeros((14, 256), F32)], axis=0
    ).astype(BF)
    w_in[2048:2064] = jnp.concatenate(
        [flat(firsts[2], 4, 2), flat(firsts[3], 4, 2), jnp.zeros((14, 128), F32)], axis=0
    ).astype(BF)
    s_up[...] = flat(firsts[4] + firsts[5], 64)


def piece_refs(refs):
    return list(refs[:4]) + [refs[4].at[k] for k in range(4)]


def pool_kernel(*refs):
    pieces, (w_own, w_other, pool_w, out, mine, padded, w_in) = piece_refs(refs), refs[5:]
    x, c, whose = lax.axis_index("x"), lax.axis_index("c"), owners()
    first = pl.ds(pl.multiple_of(c * 512, 512), 512)

    @pl.when(c == 0)
    def _():
        w_in[:, :64] = w_own[:, :64]
        w_in[:, 64:] = w_other[:, 64:]

    @pl.when(c == 1)
    def _():
        w_in[:, :64] = w_other[:, :64]
        w_in[:, 64:] = w_own[:, 64:]

    tail = w_in[2048:2064].astype(F32)
    s_in = tail[0:1] + tail[1:2]
    padded[0:128] = jnp.zeros((128, 128), BF)
    padded[128 + SEQ :] = jnp.zeros((128, 128), BF)

    @pl.loop(0, 4)
    def _(block):
        rows = pl.ds(pl.multiple_of(block * 256, 256), 256)
        total = jnp.zeros((256, 128), F32)
        squares = jnp.zeros((256, 128), F32)
        for k, piece in enumerate(pieces):
            values = piece[rows, :]
            total += dot(values, w_in[pl.ds(pl.multiple_of(whose[k] * 256, 256), 256), :])
            wide = values.astype(F32)
            wide = wide * wide
            squares += wide[:, :128] + wide[:, 128:]
        scale = lax.rsqrt(jnp.sum(squares, axis=1, keepdims=True) / 2048 + EPS)
        padded[pl.ds(pl.multiple_of(128 + block * 256, 128), 256), :] = (total * scale * s_in).astype(BF)

    half = jnp.left_shift(1, x)
    row = lax.broadcasted_iota(jnp.int32, (256, 512), 0)
    source = lax.broadcasted_iota(jnp.int32, (256, 512), 1) - 128
    band = jnp.where((source >= row - half) & (source < row + half), 1.0, 0.0).astype(BF)
    own = pool_w[x]

    @pl.loop(0, 4)
    def _(block):
        sums = dot(band, padded[pl.ds(pl.multiple_of(block * 256, 256), 512), :])
        at = lax.broadcasted_iota(jnp.int32, (256, 128), 0) + block * 256
        counts = jnp.minimum(at + half, SEQ) - jnp.maximum(at - half, 0)
        here = padded[pl.ds(pl.multiple_of(128 + block * 256, 128), 256), :].astype(F32)
        pooled = (sums / counts.astype(F32) - here).astype(BF)
        out[pl.ds(pl.multiple_of(block * 256, 256), 256), :] = dot(pooled, own).astype(BF)

    mine[...] = out[first, :]


def mix_kernel(*refs):
    pieces, grouped, near, across = piece_refs(refs), refs[5], refs[6:9], refs[9]
    weights = list(refs[10:14]) + [refs[14].at[k] for k in range(4)]
    mixed, own, factor = refs[15:]
    chips, whose = around(lax.axis_index("x")), owners()
    c = lax.axis_index("c")

    @pl.loop(0, 2)
    def _(block):
        rows = pl.ds(pl.multiple_of(block * 512, 512), 512)
        squares = jnp.zeros((512, 128), F32)
        left = jnp.concatenate(
            [grouped[rows, :]] + [
                jnp.where(block == c, a[...], across[k])
                for k, a in enumerate(near)
            ],
            axis=1,
        )
        for k in range(8):
            weight = jnp.concatenate(
                [weights[k][pl.ds(pl.multiple_of(chips[j] * 128, 128), 128), :] for j in range(4)],
                axis=0,
            )
            scale = weights[k][512:513, :].astype(F32) + weights[k][513:514, :].astype(F32)
            value = (pieces[k][rows, :].astype(F32) + dot(left, weight) * scale).astype(BF)
            mixed[rows, pl.ds(pl.multiple_of(whose[k] * 256, 256), 256)] = value
            if k == 0:
                own[rows, :] = value
            wide = value.astype(F32)
            wide = wide * wide
            squares += wide[:, :128] + wide[:, 128:]
        mean = jnp.sum(squares, axis=1, keepdims=True) / 2048
        factor[rows, :] = jnp.broadcast_to(lax.rsqrt(mean + EPS), (512, 128))


def up_parts_sum(mixed, parts, ys, rows, cols, total):
    zs = around(lax.axis_index("z"))
    for k, part in enumerate(parts):
        left = [
            mixed[rows, pl.ds(pl.multiple_of((4 * zs[2 * (k % 2) + i] + ys[k // 2]) * 128, 128), 128)]
            for i in range(2)
        ]
        total += dot(jnp.concatenate(left, axis=1), part[:, :, cols].reshape(256, 256))
    return total


def tile_of(step):
    rows = pl.ds(pl.multiple_of(lax.rem(step, 2) * 512, 512), 512)
    return rows, pl.ds(pl.multiple_of(lax.div(step, 2) * 256, 256), 256)


def up_near_kernel(mixed, *refs):
    parts, out = refs[:-1], refs[-1]
    ys = around(lax.axis_index("y"))
    if len(parts) == 3:
        parts = [b.at[pl.ds(2 * k, 2)] for b in parts for k in range(2)]

    @pl.loop(0, 4 * 2)
    def _(step):
        rows, cols = tile_of(step)
        out[rows, cols] = up_parts_sum(mixed, parts, ys, rows, cols, jnp.zeros((512, 256), F32))


def up_far_kernel(mixed, factor, s_up, near, b3, b4, hidden):
    ys = around(lax.axis_index("y"))[3:]

    @pl.loop(0, 4 * 2)
    def _(step):
        rows, cols = tile_of(step)
        total = up_parts_sum(mixed, (b3, b4), ys, rows, cols, near[rows, cols])
        scale = jnp.concatenate([factor[rows, :]] * 2, axis=1) * s_up[:, cols]
        value = jnp.maximum(total * scale, 0.0)
        hidden[rows, cols] = (value * value).astype(BF)


def down_kernel(steps, hidden, b0, b1, b2, b3, b4, own, other, taken):
    x, y, z = (lax.axis_index(name) for name in ("x", "y", "z"))
    core = lax.shift_right_logical(y, 1)
    y_is_own = core == lax.axis_index("c")
    low_is_own = y_is_own == (jnp.bitwise_and(y, 1) == 1)
    side = jnp.bitwise_and(y, 1)

    @pl.loop(0, len(steps))
    def _(k):
        chip = lax.rem(x + ((2 * k + 1) if len(steps) > 1 else steps[0]), 4)
        away = lax.rem(chip - z + 4, 4)
        for place, source in ((0, b0), (3, b1), (1, b2)):

            @pl.when(away == place)
            def _(source=source):
                @pl.loop(0, 4)
                def _(i):
                    taken[i] = source[i]

        @pl.when(away == 2)
        def _():
            @pl.loop(0, 2)
            def _(i):
                taken[i] = b3[i]
                taken[i + 2] = b4[i]

        @pl.loop(0, 2)
        def _(block):
            rows = pl.ds(pl.multiple_of(block * 512, 512), 512)
            for first, second, first_is_own, lane in (
                (taken[0], taken[3], y_is_own, side),
                (taken[1], taken[2], low_is_own, 1 - side),
            ):
                weight = jnp.concatenate(
                    [jnp.where(first_is_own, second, first), jnp.where(first_is_own, first, second)],
                    axis=0,
                )
                value = dot_t(hidden[rows, :], weight).astype(BF)
                lanes = pl.ds(pl.multiple_of(lane * 128, 128), 128)
                other[k, rows, lanes] = value[:, :128]
                own[k, rows, lanes] = value[:, 128:]


def along(bundle, axes):
    low, high = send(bundle, axes, 1), send(bundle, axes, -1)
    return [bundle, low, high, send(low[:2], axes, 1), send(high[2:], axes, -1)]


def three(array, axes):
    far = send(array, axes, 2)
    return [send(array, axes, 1), send(array, axes, -1), far]


def near_three(array):
    return three(array, "x")


def bf(*shape):
    return jax.ShapeDtypeStruct(shape, BF)


def f32(*shape):
    return jax.ShapeDtypeStruct(shape, F32)


def layer(
    stream, norm_gain, w_in, s_in, pool_w, w_out, s_out, ffn_gain, w_up, s_up, w_down, s_down
):
    ring_z = ("rep", "z")
    tokens = stream[0]

    near = near_three(tokens)
    pieces = [tokens] + near
    pieces.append(swapped(jnp.stack(pieces)))

    arrays = (
        norm_gain.reshape(16, 128),
        w_in.T,
        s_in[None],
        w_out,
        s_out[None],
        ffn_gain.reshape(16, 128),
        w_up,
        s_up[None],
        w_down,
        s_down[None],
    )
    packet, up, top, bottom = call(
        prep_kernel,
        (bf(152, 1024), bf(128, 1024), bf(64, 1024), bf(64, 1024)),
        [pltpu.VMEM((24, 1024), F32)]
        + [pltpu.VMEM(a.shape, F32) for a in arrays]
        + [pltpu.SemaphoreType.DMA((10,))],
        60,
        1_000_000,
        *arrays,
        in_hbm=10,
    )
    packets = [packet] + three(packet, "y")
    far_top, far_bottom = send(top, ring_z, 2), send(bottom, ring_z, -2)
    low, high = send(up, ring_z, 1), send(up, ring_z, -1)
    far = jnp.concatenate([far_top, far_bottom], axis=0)
    up_bundle = jnp.stack([up, low, high, far])
    mixer = jnp.stack([p[128:] for p in packets])
    mixers = [mixer, send(mixer, ring_z, 1), send(mixer, ring_z, -1)]
    mixers += [send(mixer[:2], ring_z, 2), send(mixer[2:], ring_z, -2)]
    up_parts = along(up_bundle, "y")
    down_parts = along(jnp.stack([p[:128] for p in packets]), ring_z)
    w_in_own, out_own, s_up_row = call(
        unpack_kernel, (bf(2064, 128), bf(528, 256), f32(1, 1024)), [], 8, 1_000_000, *mixers
    )

    w_in_other = swapped(w_in_own)
    grouped, mine = call(
        pool_kernel,
        (bf(SEQ, 128), bf(512, 128)),
        [pltpu.VMEM((SEQ + 256, 128), BF), pltpu.VMEM((2064, 128), BF)],
        16,
        800_000_000,
        *pieces,
        w_in_own,
        w_in_other,
        pool_w,
    )
    near = near_three(mine)
    across = swapped(jnp.stack(near))
    outs = [out_own] + near_three(out_own)
    outs.append(swapped(jnp.stack(outs)))
    mixed, mixed_own, factor = call(
        mix_kernel,
        (bf(SEQ, 2048), bf(SEQ, 256), f32(SEQ, 128)),
        [],
        32,
        2_200_000_000,
        *pieces,
        grouped,
        *near,
        across,
        *outs,
    )

    sums = call(
        up_near_kernel, f32(SEQ, 1024), [], 24, 3_200_000_000, mixed, *up_parts[:-2]
    )
    hidden = call(up_far_kernel, bf(SEQ, 1024), [], 24, 1_100_000_000, mixed, factor, s_up_row, sums, *up_parts[-2:])

    def block_sums(steps):
        count = len(steps)
        own, other = call(
            functools.partial(down_kernel, steps),
            (bf(count, SEQ, 256), bf(count, SEQ, 256)),
            [pltpu.VMEM((4, 128, 1024), BF)],
            32,
            1_075_000_000 * count,
            hidden,
            *down_parts,
        )
        crossed = swapped(other)
        return [own[k].astype(F32) + crossed[k].astype(F32) for k in range(count)]

    (far,) = block_sums((2,))
    from_low = send(far[:512].astype(BF), "x", 1)
    from_high = send(far[512:].astype(BF), "x", -1)
    after, before = block_sums((1, 3))
    (here,) = block_sums((0,))
    after = jnp.concatenate([after[:512] + from_low.astype(F32), after[512:]], axis=0)
    before = jnp.concatenate([before[:512], before[512:] + from_high.astype(F32)], axis=0)
    low = send(after.astype(BF), "x", 1)
    high = send(before.astype(BF), "x", -1)
    total = mixed_own.astype(F32) + here + low.astype(F32) + high.astype(F32)
    return total.astype(BF)[None]


def solution(mesh):
    finer = Mesh(
        mesh.devices.reshape(mesh.shape["rep"], 4, 4, 4, 2),
        ("rep", "z", "y", "x", "c"),
    )
    rows = ("rep", "z", "y")
    both = ("x", "c", "z", "y")
    return jax.shard_map(
        layer,
        mesh=finer,
        in_specs=(
            P(rows, None, TP),
            P(),
            P(FS, TP),
            P(both),
            P(),
            P(FS, TP),
            P(both),
            P(),
            P(FS, TP),
            P(both),
            P(TP, FS),
            P(FS),
        ),
        out_specs=P(rows, None, TP),
        check_vma=False,
    )
```

```python
import functools

import jax
import jax.numpy as jnp
from jax import lax
from jax.experimental import pallas as pl
from jax.experimental.pallas import tpu as pltpu
from jax.sharding import Mesh
from jax.sharding import PartitionSpec as P


BF = jnp.bfloat16
F32 = jnp.float32
EPS = 0.25
SEQ = 1024
FS = ("z", "y")
TP = ("x", "c")
VMEM = pl.BlockSpec(memory_space=pltpu.VMEM)


def send(array, axes, shift):
    count = lax.axis_size(axes)
    return lax.ppermute(array, axes, [(i, (i + shift) % count) for i in range(count)])


def swapped(array):
    return send(array, "c", 1)


def two_parts(values):
    high = values.astype(BF).astype(F32)
    return high, values - high


def dot(a, b):
    return jnp.dot(a, b, preferred_element_type=F32)


def dot_t(a, b):
    return lax.dot_general(a, b, (((1,), (1,)), ((), ())), preferred_element_type=F32)


def around(at):
    return [at] + [lax.rem(at + step, 4) for step in (3, 1, 2)]


def owners():
    x, c = lax.axis_index("x"), lax.axis_index("c")
    return [2 * chip + c for chip in around(x)] + [2 * chip + 1 - c for chip in around(x)]


def call(kernel, out_shape, scratch, limit_mb, flops, *args, in_hbm=0):
    moved = sum(a.size * a.dtype.itemsize for a in args)
    return pl.pallas_call(
        kernel,
        out_shape=out_shape,
        in_specs=[VMEM] * (len(args) - in_hbm) + [pl.BlockSpec(memory_space=pltpu.HBM)] * in_hbm,
        out_specs=jax.tree.map(lambda _: VMEM, out_shape),
        scratch_shapes=scratch,
        compiler_params=pltpu.CompilerParams(vmem_limit_bytes=limit_mb << 20),
        cost_estimate=pl.CostEstimate(flops=flops, bytes_accessed=moved, transcendentals=0),
    )(*args)


def column_of(row):
    return jnp.broadcast_to(row, (128, 128)).T


def prep_kernel(
    norm_gain_at, w_in_at, s_in_at, w_out_at, s_out_at, ffn_gain_at, w_up_at, s_up_at, w_down_at, s_down_at,
    packet, up, mixer, down, small, norm_gain, w_in, s_in, w_out, s_out, ffn_gain, w_up, s_up, w_down, s_down, done,
):
    sources = (norm_gain_at, w_in_at, s_in_at, w_out_at, s_out_at, s_up_at, ffn_gain_at, w_up_at, w_down_at, s_down_at)
    targets = (norm_gain, w_in, s_in, w_out, s_out, s_up, ffn_gain, w_up, w_down, s_down)
    copies = [pltpu.make_async_copy(a, b, done.at[k]) for k, (a, b) in enumerate(zip(sources, targets))]
    for copy in copies:
        copy.start()
    for copy in copies[:6]:
        copy.wait()
    f = 4 * lax.axis_index("z") + lax.axis_index("y")
    own = jnp.concatenate([w_in[...]] * 2, axis=0).T * column_of(norm_gain[pl.ds(f, 1), :])
    low_lanes = lax.broadcasted_iota(jnp.int32, (8, 128), 1) < 64
    for j in range(8):
        lanes = slice(j * 128, j * 128 + 128)
        small[0:8, lanes] = jnp.where(low_lanes, own[j * 16 : j * 16 + 8], own[j * 16 + 8 : j * 16 + 16])
    for j in range(4):
        small[8:16, j * 256 : j * 256 + 256] = w_out[j * 8 : j * 8 + 8, :]
    small[16:24] = jnp.zeros((8, 1024), F32)
    for row, at in ((s_out[...], 0), (s_in[...], 256), (s_up[...], 512)):
        high, low = two_parts(row)
        small[16:17, at : at + row.shape[1]] = high
        small[16:17, at + 128 : at + 128 + row.shape[1]] = low
    mixer[...] = small[...].astype(BF)
    packet[128:] = mixer[...]
    for copy in copies[6:]:
        copy.wait()
    gain = column_of(ffn_gain[pl.ds(f, 1), :])
    for j in range(8):
        lanes = slice(j * 128, j * 128 + 128)
        up[:, lanes] = (w_up[:, lanes] * gain).astype(BF)
        down[:, lanes] = (w_down[lanes, :] * s_down[...]).T.astype(BF)
    packet[:128] = down[...]


def unpack_kernel(m0, m1, m2, m3, w_in, w_out, s_up):
    ys, zs = around(lax.axis_index("y")), around(lax.axis_index("z"))
    lane = lax.broadcasted_iota(jnp.int32, (16, 128), 1)
    at = lax.broadcasted_iota(jnp.int32, (16, 128), 0)
    low_lanes = lane[:8] < 64
    firsts = [jnp.zeros((16, 128), F32) for _ in range(6)]
    for p, zz in enumerate(zs):
        for k, yy in enumerate(ys):
            f = 4 * zz + yy
            block = (m0, m1, m2, m3)[p][k].astype(F32)
            for j in range(8):
                part = block[:8, j * 128 : j * 128 + 128]
                turned = pltpu.roll(part, 64, 1)
                rows = jnp.concatenate(
                    [jnp.where(low_lanes, part, turned), jnp.where(low_lanes, turned, part)], axis=0
                )
                w_in[pl.ds(pl.multiple_of(f * 128 + j * 16, 16), 16), :] = rows.astype(BF)
            rows = jnp.concatenate([block[8:16, j * 256 : j * 256 + 256] for j in range(4)], axis=0)
            w_out[pl.ds(pl.multiple_of(f * 32, 32), 32), :] = rows.astype(BF)
            for j in range(6):
                row = jnp.broadcast_to(block[16:17, j * 128 : j * 128 + 128], (16, 128))
                firsts[j] = jnp.where(at == f, row, firsts[j])

    def flat(rows, width, copies=1):
        pieces = []
        count = min(16, 128 // width)
        for group in range(16 // count):
            total = jnp.zeros((1, 128), F32)
            for i in range(count):
                source = group * count + i
                row = jnp.where(lane[:1] < width, rows[source : source + 1], 0.0)
                for again in range(copies):
                    shift = i * width + 64 * again
                    total += pltpu.roll(row, shift, 1) if shift else row
            pieces.append(total)
        return jnp.concatenate(pieces, axis=1) if len(pieces) > 1 else pieces[0]

    w_out[512:528] = jnp.concatenate(
        [flat(firsts[0], 16), flat(firsts[1], 16), jnp.zeros((14, 256), F32)], axis=0
    ).astype(BF)
    w_in[2048:2064] = jnp.concatenate(
        [flat(firsts[2], 4, 2), flat(firsts[3], 4, 2), jnp.zeros((14, 128), F32)], axis=0
    ).astype(BF)
    s_up[...] = flat(firsts[4] + firsts[5], 64)


def piece_refs(refs):
    return list(refs[:4]) + [refs[4].at[k] for k in range(4)]


def pool_kernel(*refs):
    pieces, (w_own, w_other, pool_w, out, mine, padded, w_in) = piece_refs(refs), refs[5:]
    x, c, whose = lax.axis_index("x"), lax.axis_index("c"), owners()
    first = pl.ds(pl.multiple_of(c * 512, 512), 512)

    @pl.when(c == 0)
    def _():
        w_in[:, :64] = w_own[:, :64]
        w_in[:, 64:] = w_other[:, 64:]

    @pl.when(c == 1)
    def _():
        w_in[:, :64] = w_other[:, :64]
        w_in[:, 64:] = w_own[:, 64:]

    tail = w_in[2048:2064].astype(F32)
    s_in = tail[0:1] + tail[1:2]
    padded[0:128] = jnp.zeros((128, 128), BF)
    padded[128 + SEQ :] = jnp.zeros((128, 128), BF)

    @pl.loop(0, 4)
    def _(block):
        rows = pl.ds(pl.multiple_of(block * 256, 256), 256)
        total = jnp.zeros((256, 128), F32)
        squares = jnp.zeros((256, 128), F32)
        for k, piece in enumerate(pieces):
            values = piece[rows, :]
            total += dot(values, w_in[pl.ds(pl.multiple_of(whose[k] * 256, 256), 256), :])
            wide = values.astype(F32)
            wide = wide * wide
            squares += wide[:, :128] + wide[:, 128:]
        scale = lax.rsqrt(jnp.sum(squares, axis=1, keepdims=True) / 2048 + EPS)
        padded[pl.ds(pl.multiple_of(128 + block * 256, 128), 256), :] = (total * scale * s_in).astype(BF)

    half = jnp.left_shift(1, x)
    row = lax.broadcasted_iota(jnp.int32, (256, 512), 0)
    source = lax.broadcasted_iota(jnp.int32, (256, 512), 1) - 128
    band = jnp.where((source >= row - half) & (source < row + half), 1.0, 0.0).astype(BF)
    own = pool_w[x]

    @pl.loop(0, 4)
    def _(block):
        sums = dot(band, padded[pl.ds(pl.multiple_of(block * 256, 256), 512), :])
        at = lax.broadcasted_iota(jnp.int32, (256, 128), 0) + block * 256
        counts = jnp.minimum(at + half, SEQ) - jnp.maximum(at - half, 0)
        here = padded[pl.ds(pl.multiple_of(128 + block * 256, 128), 256), :].astype(F32)
        pooled = (sums / counts.astype(F32) - here).astype(BF)
        out[pl.ds(pl.multiple_of(block * 256, 256), 256), :] = dot(pooled, own).astype(BF)

    mine[...] = out[first, :]


def mix_kernel(*refs):
    pieces, grouped, near, across = piece_refs(refs), refs[5], refs[6:9], refs[9]
    weights = list(refs[10:14]) + [refs[14].at[k] for k in range(4)]
    mixed, own, factor = refs[15:]
    chips, whose = around(lax.axis_index("x")), owners()
    c = lax.axis_index("c")

    @pl.loop(0, 2)
    def _(block):
        rows = pl.ds(pl.multiple_of(block * 512, 512), 512)
        squares = jnp.zeros((512, 128), F32)
        left = jnp.concatenate(
            [grouped[rows, :]] + [
                jnp.where(block == c, a[...], across[k])
                for k, a in enumerate(near)
            ],
            axis=1,
        )
        for k in range(8):
            weight = jnp.concatenate(
                [weights[k][pl.ds(pl.multiple_of(chips[j] * 128, 128), 128), :] for j in range(4)],
                axis=0,
            )
            scale = weights[k][512:513, :].astype(F32) + weights[k][513:514, :].astype(F32)
            value = (pieces[k][rows, :].astype(F32) + dot(left, weight) * scale).astype(BF)
            mixed[rows, pl.ds(pl.multiple_of(whose[k] * 256, 256), 256)] = value
            if k == 0:
                own[rows, :] = value
            wide = value.astype(F32)
            wide = wide * wide
            squares += wide[:, :128] + wide[:, 128:]
        mean = jnp.sum(squares, axis=1, keepdims=True) / 2048
        factor[rows, :] = jnp.broadcast_to(lax.rsqrt(mean + EPS), (512, 128))


def up_parts_sum(mixed, parts, ys, rows, cols, total):
    zs = around(lax.axis_index("z"))
    for k, part in enumerate(parts):
        left = [
            mixed[rows, pl.ds(pl.multiple_of((4 * zs[2 * (k % 2) + i] + ys[k // 2]) * 128, 128), 128)]
            for i in range(2)
        ]
        total += dot(jnp.concatenate(left, axis=1), part[:, :, cols].reshape(256, 256))
    return total


def tile_of(step):
    rows = pl.ds(pl.multiple_of(lax.rem(step, 2) * 512, 512), 512)
    return rows, pl.ds(pl.multiple_of(lax.div(step, 2) * 256, 256), 256)


def up_near_kernel(mixed, *refs):
    parts, out = refs[:-1], refs[-1]
    ys = around(lax.axis_index("y"))
    if len(parts) == 3:
        parts = [b.at[pl.ds(2 * k, 2)] for b in parts for k in range(2)]

    @pl.loop(0, 4 * 2)
    def _(step):
        rows, cols = tile_of(step)
        out[rows, cols] = up_parts_sum(mixed, parts, ys, rows, cols, jnp.zeros((512, 256), F32))


def up_far_kernel(mixed, factor, s_up, near, b3, b4, hidden):
    ys = around(lax.axis_index("y"))[3:]

    @pl.loop(0, 4 * 2)
    def _(step):
        rows, cols = tile_of(step)
        total = up_parts_sum(mixed, (b3, b4), ys, rows, cols, near[rows, cols])
        scale = jnp.concatenate([factor[rows, :]] * 2, axis=1) * s_up[:, cols]
        value = jnp.maximum(total * scale, 0.0)
        hidden[rows, cols] = (value * value).astype(BF)


def down_kernel(steps, hidden, *refs):
    parts, (own, other, taken) = refs[:8], refs[8:]
    x, y, z = (lax.axis_index(name) for name in ("x", "y", "z"))
    core = lax.shift_right_logical(y, 1)
    y_is_own = core == lax.axis_index("c")
    low_is_own = y_is_own == (jnp.bitwise_and(y, 1) == 1)
    side = jnp.bitwise_and(y, 1)

    @pl.loop(0, len(steps))
    def _(k):
        chip = lax.rem(x + ((2 * k + 1) if len(steps) > 1 else steps[0]), 4)
        away = lax.rem(chip - z + 4, 4)
        for k_place, place in enumerate((0, 3, 1, 2)):

            @pl.when(away == place)
            def _(k_place=k_place):
                @pl.loop(0, 2)
                def _(i):
                    taken[i] = parts[2 * k_place][i]
                    taken[i + 2] = parts[2 * k_place + 1][i]

        @pl.loop(0, 2)
        def _(block):
            rows = pl.ds(pl.multiple_of(block * 512, 512), 512)
            for first, second, first_is_own, lane in (
                (taken[0], taken[3], y_is_own, side),
                (taken[1], taken[2], low_is_own, 1 - side),
            ):
                weight = jnp.concatenate(
                    [jnp.where(first_is_own, second, first), jnp.where(first_is_own, first, second)],
                    axis=0,
                )
                value = dot_t(hidden[rows, :], weight).astype(BF)
                lanes = pl.ds(pl.multiple_of(lane * 128, 128), 128)
                other[k, rows, lanes] = value[:, :128]
                own[k, rows, lanes] = value[:, 128:]


def along(bundle, axes):
    low, high = send(bundle, axes, 1), send(bundle, axes, -1)
    return [bundle, low, high, send(low[:2], axes, 1), send(high[2:], axes, -1)]


def three(array, axes):
    far = send(array, axes, 2)
    return [send(array, axes, 1), send(array, axes, -1), far]


def near_three(array):
    return three(array, "x")


def bf(*shape):
    return jax.ShapeDtypeStruct(shape, BF)


def f32(*shape):
    return jax.ShapeDtypeStruct(shape, F32)


def layer(
    stream, norm_gain, w_in, s_in, pool_w, w_out, s_out, ffn_gain, w_up, s_up, w_down, s_down
):
    ring_z = ("rep", "z")
    tokens = stream[0]

    near = near_three(tokens)
    pieces = [tokens] + near
    pieces.append(swapped(jnp.stack(pieces)))

    arrays = (
        norm_gain.reshape(16, 128),
        w_in.T,
        s_in[None],
        w_out,
        s_out[None],
        ffn_gain.reshape(16, 128),
        w_up,
        s_up[None],
        w_down,
        s_down[None],
    )
    packet, up, mixer, down = call(
        prep_kernel,
        (bf(152, 1024), bf(128, 1024), bf(24, 1024), bf(128, 1024)),
        [pltpu.VMEM((24, 1024), F32)]
        + [pltpu.VMEM(a.shape, F32) for a in arrays]
        + [pltpu.SemaphoreType.DMA((10,))],
        60,
        1_000_000,
        *arrays,
        in_hbm=10,
    )
    packets = three(packet, "y")
    far = send(up, ring_z, 2)
    up_bundle = jnp.stack([up, send(up, ring_z, 1), send(up, ring_z, -1), far])
    mixer = jnp.stack([mixer] + [p[128:] for p in packets])
    far = send(mixer, ring_z, -2)
    mixers = [mixer, send(mixer, ring_z, 1), send(mixer, ring_z, -1), far]
    up_parts = along(up_bundle, "y")
    top = jnp.stack([down, packets[0][:128]])
    bottom = jnp.stack([packets[1][:128], packets[2][:128]])
    low_top, high_bottom = send(top, ring_z, 1), send(bottom, ring_z, -1)
    low_bottom, high_top = send(bottom, ring_z, 1), send(top, ring_z, -1)
    far_top, far_bottom = send(low_top, ring_z, 1), send(high_bottom, ring_z, -1)
    down_parts = [top, bottom, low_top, low_bottom, high_top, high_bottom, far_top, far_bottom]
    w_in_own, out_own, s_up_row = call(
        unpack_kernel, (bf(2064, 128), bf(528, 256), f32(1, 1024)), [], 8, 1_000_000, *mixers
    )

    w_in_other = swapped(w_in_own)
    grouped, mine = call(
        pool_kernel,
        (bf(SEQ, 128), bf(512, 128)),
        [pltpu.VMEM((SEQ + 256, 128), BF), pltpu.VMEM((2064, 128), BF)],
        16,
        800_000_000,
        *pieces,
        w_in_own,
        w_in_other,
        pool_w,
    )
    near = near_three(mine)
    across = swapped(jnp.stack(near))
    outs = [out_own] + near_three(out_own)
    outs.append(swapped(jnp.stack(outs)))
    mixed, mixed_own, factor = call(
        mix_kernel,
        (bf(SEQ, 2048), bf(SEQ, 256), f32(SEQ, 128)),
        [],
        32,
        2_200_000_000,
        *pieces,
        grouped,
        *near,
        across,
        *outs,
    )

    sums = call(
        up_near_kernel, f32(SEQ, 1024), [], 24, 3_200_000_000, mixed, *up_parts[:-2]
    )
    hidden = call(up_far_kernel, bf(SEQ, 1024), [], 24, 1_100_000_000, mixed, factor, s_up_row, sums, *up_parts[-2:])

    def block_sums(steps):
        count = len(steps)
        own, other = call(
            functools.partial(down_kernel, steps),
            (bf(count, SEQ, 256), bf(count, SEQ, 256)),
            [pltpu.VMEM((4, 128, 1024), BF)],
            32,
            1_075_000_000 * count,
            hidden,
            *down_parts,
        )
        crossed = swapped(other)
        return [own[k].astype(F32) + crossed[k].astype(F32) for k in range(count)]

    (far,) = block_sums((2,))
    from_low = send(far[:512].astype(BF), "x", 1)
    from_high = send(far[512:].astype(BF), "x", -1)
    after, before = block_sums((1, 3))
    (here,) = block_sums((0,))
    after = jnp.concatenate([after[:512] + from_low.astype(F32), after[512:]], axis=0)
    before = jnp.concatenate([before[:512], before[512:] + from_high.astype(F32)], axis=0)
    low = send(after.astype(BF), "x", 1)
    high = send(before.astype(BF), "x", -1)
    total = mixed_own.astype(F32) + here + low.astype(F32) + high.astype(F32)
    return total.astype(BF)[None]


def solution(mesh):
    finer = Mesh(
        mesh.devices.reshape(mesh.shape["rep"], 4, 4, 4, 2),
        ("rep", "z", "y", "x", "c"),
    )
    rows = ("rep", "z", "y")
    both = ("x", "c", "z", "y")
    return jax.shard_map(
        layer,
        mesh=finer,
        in_specs=(
            P(rows, None, TP),
            P(),
            P(FS, TP),
            P(both),
            P(),
            P(FS, TP),
            P(both),
            P(),
            P(FS, TP),
            P(both),
            P(TP, FS),
            P(FS),
        ),
        out_specs=P(rows, None, TP),
        check_vma=False,
    )
```
